512 devices in a mesh: fs: 64 (over z, y), tp: 8 (over x, core).
Axes of the slice: x: 4, y: 4, z: 16, core: 2. Of those that a mesh axis runs over, the one named last changes fastest.
Arguments:
- normed_input: bfloat16 [32768, 4096], P('fs', 'tp'), may hold values from -16 to 16
- value_cotangent: bfloat16 [32768, 2048], P('fs', 'tp'), may hold values from -0.005859375 to 0.005859375
- mixer_output: bfloat16 [32768, 2048], P('fs', 'tp'), may hold values from -6 to 6
- output_cotangent: bfloat16 [32768, 4096], P('fs', 'tp'), may hold values from -0.0078125 to 0.0078125
- value_factor: bfloat16 [4096, 128], replicated, may hold values from -0.5 to 0.5
- output_factor: bfloat16 [2048, 128], replicated, may hold values from -0.5 to 0.5
- value_master: float32 [4096, 2048], P('fs', 'tp'), may hold values from -0.09375 to 0.09375
- value_moment: float32 [128, 2048], P(None, 'tp'), may hold values from -6 to 6
- value_second: float32 [128, 2048], P(None, 'tp'), may hold values from 0.0625 to 16, as said below
- output_master: float32 [2048, 4096], P('fs', 'tp'), may hold values from -0.125 to 0.125
- output_moment: float32 [128, 4096], P(None, 'tp'), may hold values from -6 to 6
- output_second: float32 [128, 4096], P(None, 'tp'), may hold values from 0.0625 to 16, as said below
Outputs:
- value_step: float32 [4096, 2048], P('fs', 'tp')
- value_new: float32 [4096, 2048], P('fs', 'tp')
- value_copy: bfloat16 [4096, 2048], P(None, 'tp')
- value_moment_new: float32 [128, 2048], P(None, 'tp')
- value_second_new: float32 [128, 2048], P(None, 'tp')
- output_step: float32 [2048, 4096], P('fs', 'tp')
- output_new: float32 [2048, 4096], P('fs', 'tp')
- output_copy: bfloat16 [2048, 4096], P(None, 'tp')
- output_moment_new: float32 [128, 4096], P(None, 'tp')
- output_second_new: float32 [128, 4096], P(None, 'tp')
The draws below stay inside these ranges and needn't reach their ends.
Inputs may be any that keep to these rules, and one draw needn't show every extreme that they name: `value_second`: positive, with a scale that differs between groups of columns. `output_second`: positive, with a scale that differs between groups of columns.
All inputs are finite; a program needn't handle non-finite values.
Results may differ from the reference program's by a relative error of at most 0.004.
Values may be sent and summed in bfloat16 or wider, within the bound.
A program may use at most 64 MiB of HBM per device.

```python
import math
import jax
import jax.numpy as jnp
from jax import lax

D = 4096
WIDTH = 2048
R = 128
TOK_DEV = 512
TOKENS = 32768
N_FS = 64
N_TP = 8


def second_draw(key, rows, columns):
    levels = jnp.exp(jax.random.uniform(jax.random.fold_in(key, 11), (rows, columns), jnp.float32, math.log(0.25), math.log(4.0)))
    groups = jnp.exp(jax.random.uniform(jax.random.fold_in(key, 12), (16,), jnp.float32, math.log(0.25), math.log(4.0)))
    return levels * jnp.repeat(groups, columns // 16)[None, :]


def draw_value_second(key, part):
    return second_draw(jax.random.fold_in(key, 1), R, WIDTH)


def draw_output_second(key, part):
    return second_draw(jax.random.fold_in(key, 2), R, D)


def strengthened(array, rng, source, target, parts, factor):
    def block_of(axis_at):
        return (jnp.arange(array.shape[axis_at]) // (array.shape[axis_at] // parts)).reshape((-1,) + (1,) * (array.ndim - 1 - axis_at))

    near = jax.random.permutation(rng, parts)[block_of(target)]
    other_side = (block_of(target) + parts // 2) % parts
    return jnp.where((block_of(source) == near) | (block_of(source) == other_side), factor * array, array)


def block_levels(own_key, extent, split, least, top_value):
    def one(axis_at, parts):
        draws = jax.random.uniform(jax.random.fold_in(jax.random.fold_in(own_key, 6), axis_at), (parts,), jnp.float32, least / len(split), top_value / len(split))
        return jnp.repeat(jnp.exp(draws), extent[axis_at] // parts).reshape((-1,) + (1,) * (len(extent) - axis_at - 1))

    factor_of = one(*split[0])
    for cut in split[1:]:
        factor_of = factor_of * one(*cut)
    return factor_of


def noise(key, extent, width, reach, pieces=(), dtype=jnp.bfloat16):
    result = width * jax.random.normal(key, extent, jnp.float32)
    if pieces:
        result = result * block_levels(key, extent, pieces, -0.22, 0.18)
    return jnp.clip(result, -reach, reach).astype(dtype)


def gaussian_with(key, dims, scale, bound, shards, heavy, held_as=jnp.bfloat16):
    array = scale * jax.random.normal(key, dims, jnp.float32)
    if shards:
        array = array * block_levels(key, dims, shards, -0.22, 0.18)
    return jnp.clip(strengthened(array, jax.random.fold_in(key, 3), *heavy), -bound, bound).astype(held_as)


def setup_inputs(seed: int = 0) -> dict:
    streams_of = jax.random.split(jax.random.key(seed), 13)
    return {
        "normed_input": gaussian_with(streams_of[0], (TOKENS, D), 1.0, 16.0, ((0, 64), (1, 8)), (0, 1, 64, 4.0)),
        "value_cotangent": noise(streams_of[1], (TOKENS, WIDTH), ((R / (D * TOK_DEV * N_FS)) ** 0.5), 0.005859375, ((0, 64), (1, 8))),
        "mixer_output": noise(streams_of[2], (TOKENS, WIDTH), 1.0, 6.0, ((0, 64), (1, 8))),
        "output_cotangent": noise(streams_of[3], (TOKENS, D), ((R / (WIDTH * TOK_DEV * N_FS)) ** 0.5), 0.0078125, ((0, 64), (1, 8))),
        "value_factor": noise(streams_of[4], (D, R), R ** -0.5, 0.5),
        "output_factor": noise(streams_of[5], (WIDTH, R), R ** -0.5, 0.5),
        "value_master": noise(streams_of[6], (D, WIDTH), D ** -0.5, 0.09375, ((0, 64), (1, 8)), jnp.float32),
        "value_moment": noise(streams_of[7], (R, WIDTH), 1.0, 6.0, ((1, 8),), jnp.float32),
        "value_second": draw_value_second(jax.random.fold_in(streams_of[12], 71), 0),
        "output_master": noise(streams_of[9], (WIDTH, D), WIDTH ** -0.5, 0.125, ((0, 64), (1, 8)), jnp.float32),
        "output_moment": noise(streams_of[10], (R, D), 1.0, 6.0, ((1, 8),), jnp.float32),
        "output_second": draw_output_second(jax.random.fold_in(streams_of[12], 71), 0),
    }


BETA_ONE = 0.8
BETA_TWO = 0.9
EPSILON = 1e-08
STEP_RATE = 0.005
FLOOR = 0.25

def moments(first, second, projected):
    first_new = BETA_ONE * first + (1.0 - BETA_ONE) * projected
    second_new = BETA_TWO * second + (1.0 - BETA_TWO) * projected * projected
    normalized = first_new / (jnp.sqrt(second_new) + EPSILON)
    return (first_new, second_new, normalized)

def reference(normed_input, value_cotangent, mixer_output, output_cotangent, value_factor, output_factor, value_master, value_moment, value_second, output_master, output_moment, output_second):
    highest = lax.Precision.HIGHEST
    input_reduced = jnp.dot(normed_input.astype(jnp.float32), value_factor.astype(jnp.float32), precision=highest)
    value_projected = jnp.dot(input_reduced.T, value_cotangent.astype(jnp.float32), precision=highest)
    split_cols = WIDTH // N_TP
    mixer_blocks = mixer_output.astype(jnp.float32).reshape(TOKENS, N_TP, split_cols)
    factor_blocks = output_factor.astype(jnp.float32).reshape(N_TP, split_cols, R)
    partials = jnp.einsum('tnc,ncr->ntr', mixer_blocks, factor_blocks, precision=highest).astype(jnp.bfloat16)
    partials = lax.optimization_barrier(partials)
    mixer_reduced = lax.optimization_barrier(jnp.sum(partials.astype(jnp.float32), axis=0)).astype(jnp.bfloat16)
    output_projected = jnp.dot(mixer_reduced.astype(jnp.float32).T, output_cotangent.astype(jnp.float32), precision=highest)
    value_moment_new, value_second_new, value_norm = moments(value_moment, value_second, value_projected)
    output_moment_new, output_second_new, output_norm = moments(output_moment, output_second, output_projected)
    value_scale = lax.rsqrt(jnp.mean(value_norm * value_norm) + FLOOR)
    output_scale = lax.rsqrt(jnp.mean(output_norm * output_norm) + FLOOR)
    value_step = value_scale * jnp.dot(value_factor.astype(jnp.float32), value_norm, precision=highest)
    output_step = output_scale * jnp.dot(output_factor.astype(jnp.float32), output_norm, precision=highest)
    value_new = value_master - STEP_RATE * value_step
    output_new = output_master - STEP_RATE * output_step
    return (value_step, value_new, value_new.astype(jnp.bfloat16), value_moment_new, value_second_new, output_step, output_new, output_new.astype(jnp.bfloat16), output_moment_new, output_second_new)
```

```python
import jax
import jax.numpy as jnp
from jax import lax
from jax.experimental import pallas as pl
from jax.experimental.pallas import tpu as pltpu
from jax.sharding import Mesh
from jax.sharding import PartitionSpec as P

D = 4096
WIDTH = 2048
R = 128
TOK = 512
NZ, NY, NT = 16, 4, 8
FEAT = D // NT
HEAD = WIDTH // NT
VC = WIDTH // NT
OC = D // NT
PC = VC + OC
VROWS = D // (NZ * NY)
OROWS = WIDTH // (NZ * NY)
BLK = VROWS + 2 * OROWS
ASPLIT = 48
BHALF = 96

BETA_ONE = 0.8
BETA_TWO = 0.9
EPSILON = 1e-08
STEP_RATE = 0.005
FLOOR = 0.25

BF = jnp.bfloat16
F32 = jnp.float32
MESH = pl.DeviceIdType.MESH


def moments(first, second, projected):
    first_new = BETA_ONE * first + (1.0 - BETA_ONE) * projected
    second_new = BETA_TWO * second + (1.0 - BETA_TWO) * projected * projected
    normalized = first_new / (jnp.sqrt(second_new) + EPSILON)
    return first_new, second_new, normalized


def exchange_kernel(
    n_in, vc_in, mo_in, oc_in, fv_in, fo_in, vw_in, vm_in, vs_in, ow_in, om_in, os_in,
    g_out, p_out, s_out,
    nb, vcb, mob, ocb, fvb, fob, vwb, vmb, vsb, owb, omb, osb,
    xs, xr, xg, pf, pb, yr, zs, zb, zr, zg, nat, yg, st, sr, g,
    lsem, osem,
    xs_s, xs_r, xg_s, xg_r, sc_s, sc_r, yr_s, yr_r, yg_s, yg_r,
    zr_s, zr_r, zg_s, zg_r, ay_s, ay_r, az_s, az_r, bz_s, bz_r, by_s, by_r,
):
    z, y, t = lax.axis_index("z"), lax.axis_index("y"), lax.axis_index("tp")

    def around(k, i, n):
        return lax.rem(k + (i + n), n)

    barrier = pltpu.get_barrier_semaphore()
    for i in range(1, NT):
        pl.semaphore_signal(barrier, inc=1, device_id={"tp": around(t, i, NT)}, device_id_type=MESH)
    for i in range(1, NY):
        pl.semaphore_signal(barrier, inc=1, device_id={"y": around(y, i, NY)}, device_id_type=MESH)
    for i in range(1, NZ):
        pl.semaphore_signal(barrier, inc=1, device_id={"z": around(z, i, NZ)}, device_id_type=MESH)

    loads = []
    for k, (src, dst) in enumerate((
        (vw_in, vwb), (ow_in, owb),
        (fv_in.at[pl.ds(pl.multiple_of(t * FEAT, FEAT), FEAT)], fvb), (n_in, nb),
        (fo_in.at[pl.ds(pl.multiple_of(t * HEAD, HEAD), HEAD)], fob), (mo_in, mob),
        (vc_in, vcb), (oc_in, ocb),
        (vm_in, vmb), (vs_in, vsb), (om_in, omb), (os_in, osb),
    )):
        c = pltpu.make_async_copy(src, dst, lsem.at[k])
        c.start()
        loads.append(c)

    sent = []

    def remote(src, dst, ssem, rsem, **where):
        c = pltpu.make_async_remote_copy(
            src_ref=src, dst_ref=dst, send_sem=ssem, recv_sem=rsem,
            device_id=where, device_id_type=MESH,
        )
        return c

    def send(src, dst, ssem, rsem, **where):
        c = remote(src, dst, ssem, rsem, **where)
        c.start()
        sent.append(c)

    def arrived(dst, rsem):
        remote(dst, dst, rsem, rsem, tp=t).wait_recv()

    for c in loads[:2]:
        c.wait()
    g[z, y, 0:VROWS, :] = vwb[...].astype(BF)
    g[z, y, VROWS:VROWS + OROWS, :] = owb[:, 0:VC].astype(BF)
    g[z, y, VROWS + OROWS:BLK, :] = owb[:, VC:OC].astype(BF)
    for c in loads[2:4]:
        c.wait()
    nt = (((1,), (1,)), ((), ()))
    part = lax.dot_general(fvb[...].T, nb[...], nt, preferred_element_type=F32)
    xs[:, 0:16, :] = part.astype(BF).reshape(NT, 16, TOK)
    for c in loads[4:6]:
        c.wait()
    part = lax.dot_general(fob[...].T, mob[...], nt, preferred_element_type=F32)
    xs[:, 16:32, :] = part.astype(BF).reshape(NT, 16, TOK)

    def a_rows(k, ys=None):
        return g.at[k, :, pl.ds(0, ASPLIT), :] if ys is None else g.at[k, pl.ds(ys, NY // 2), pl.ds(0, ASPLIT), :]

    def b_rows(k, j=None, part=None):
        lo, hi = {None: (ASPLIT, BLK), 0: (ASPLIT, BHALF), 1: (BHALF, BLK)}[part]
        return g.at[k, y if j is None else j, pl.ds(lo, hi - lo), :]

    LAST = NZ // 2
    up, down = around(z, 1, NZ), around(z, -1, NZ)
    yup, ydown = around(y, 1, NY), around(y, -1, NY)

    def a_begin():
        own = g.at[z, y, pl.ds(0, ASPLIT), :]
        for i in range(1, NY):
            send(own, own, ay_s.at[i], ay_r.at[i], y=around(y, i, NY))

    def a_ring(s):
        if s == 0:
            for i in range(1, NY):
                arrived(g.at[z, around(y, -i, NY), pl.ds(0, ASPLIT), :], ay_r.at[i])
        below, above = around(z, -s, NZ), around(z, s, NZ)
        if 0 < s < LAST:
            arrived(a_rows(below), az_r.at[0, s])
            arrived(a_rows(above), az_r.at[1, s])
        if s == LAST:
            arrived(a_rows(below, 0), az_r.at[0, s])
            arrived(a_rows(above, NY // 2), az_r.at[1, s])
            return
        half = s + 1 == LAST
        for d, (k, to) in enumerate(((below, up), (above, down))):
            block = a_rows(k, d * (NY // 2)) if half else a_rows(k)
            send(block, block, az_s.at[d, s + 1], az_r.at[d, s + 1], z=to)

    def b_across(k, b):
        block = b_rows(k)
        send(block, block, by_s.at[0, b], by_r.at[0, b], y=yup)
        send(block, block, by_s.at[1, b], by_r.at[1, b], y=ydown)

    def b_ids(s):
        if s == 0:
            return ((0, 0),)
        if s == LAST:
            return ((LAST, NZ - 1),)
        return ((-s, 2 * s - 1), (s, 2 * s))

    def b_ring(s):
        below, above = around(z, -s, NZ), around(z, s, NZ)
        if 0 < s < LAST:
            arrived(b_rows(below), bz_r.at[0, s])
            arrived(b_rows(above), bz_r.at[1, s])
        if s == LAST:
            arrived(b_rows(below, part=0), bz_r.at[0, s])
            arrived(b_rows(above, part=1), bz_r.at[1, s])
        else:
            half = s + 1 == LAST
            for d, (k, to) in enumerate(((below, up), (above, down))):
                block = b_rows(k, part=d) if half else b_rows(k)
                send(block, block, bz_s.at[d, s + 1], bz_r.at[d, s + 1], z=to)
        for off, b in b_ids(s):
            b_across(around(z, off, NZ), b)

    def b_forward(s):
        for off, b in b_ids(s):
            k = around(z, off, NZ)
            arrived(b_rows(k, ydown), by_r.at[0, b])
            block = b_rows(k, ydown, 0)
            send(block, block, by_s.at[2, b], by_r.at[2, b], y=yup)
            arrived(b_rows(k, yup), by_r.at[1, b])
            block = b_rows(k, yup, 1)
            send(block, block, by_s.at[3, b], by_r.at[3, b], y=ydown)

    writes = []

    def b_end(s):
        across = around(y, 2, NY)
        for off, b in b_ids(s):
            k = around(z, off, NZ)
            arrived(b_rows(k, across, 0), by_r.at[2, b])
            arrived(b_rows(k, across, 1), by_r.at[3, b])
            c = pltpu.make_async_copy(g.at[k], g_out.at[k], osem.at[b])
            c.start()
            writes.append(c)

    pl.semaphore_wait(barrier, NT + NY + NZ - 3)

    def c_scatter():
        for i in range(1, NT):
            to = around(t, i, NT)
            send(xs.at[to], xr.at[i], xs_s.at[i], xs_r.at[i], tp=to)

    def c_gather():
        for i in range(1, NT):
            arrived(xr.at[i], xs_r.at[i])
        total = xs[t].astype(F32)
        for i in range(1, NT):
            total = total + xr[i].astype(F32)
        xg[t] = total.astype(BF)
        for i in range(1, NT):
            send(xg.at[t], xg.at[t], xg_s.at[i], xg_r.at[i], tp=around(t, i, NT))

    def c_project():
        for c in loads[6:8]:
            c.wait()
        for i in range(1, NT):
            arrived(xg.at[around(t, -i, NT)], xg_r.at[i])
        left = xg[:, 0:16, :].reshape(R, TOK)
        right = xg[:, 16:32, :].reshape(R, TOK)
        pv = jnp.dot(left, vcb[...], preferred_element_type=F32).reshape(NY, R // NY, VC)
        po = jnp.dot(right, ocb[...], preferred_element_type=F32).reshape(NY, R // NY, OC)
        pf[:, :, 0:VC] = pv
        pf[:, :, VC:PC] = po
        pb[:, :, 0:VC] = pv.astype(BF)
        pb[:, :, VC:PC] = po.astype(BF)
        for i in range(1, NY):
            to = around(y, i, NY)
            send(pb.at[to], yr.at[i], yr_s.at[i], yr_r.at[i], y=to)

    def c_zscatter():
        for i in range(1, NY):
            arrived(yr.at[i], yr_r.at[i])
        total = pf[y]
        for i in range(1, NY):
            total = total + yr[i].astype(F32)
        for k in range(NZ):
            q, r = divmod(k, 4)
            zs[k, 0:8, :] = total[8 * q:8 * q + 8, VC + 128 * r:VC + 128 * r + 128]
            q, r = divmod(k, 2)
            zs[k, 8:12, :] = total[4 * q:4 * q + 4, 128 * r:128 * r + 128]
            zs[k, 12:16, :] = jnp.zeros((4, 128), F32)
        zb[...] = zs[...].astype(BF)
        for i in range(1, NZ):
            to = around(z, i, NZ)
            send(zb.at[to], zr.at[i], zr_s.at[i], zr_r.at[i], z=to)

    def c_zgather():
        for i in range(1, NZ):
            arrived(zr.at[i], zr_r.at[i])
        total = zs[z]
        for i in range(1, NZ):
            total = total + zr[i].astype(F32)
        zg[z] = total.astype(BF)
        for i in range(1, NZ):
            send(zg.at[z], zg.at[z], zg_s.at[i], zg_r.at[i], z=around(z, i, NZ))

    def c_ygather():
        for i in range(1, NZ):
            arrived(zg.at[around(z, -i, NZ)], zg_r.at[i])
        for k in range(NZ):
            chunk = zg[k].astype(F32)
            q, r = divmod(k, 4)
            nat[8 * q:8 * q + 8, VC + 128 * r:VC + 128 * r + 128] = chunk[0:8]
            q, r = divmod(k, 2)
            nat[4 * q:4 * q + 4, 128 * r:128 * r + 128] = chunk[8:12]
        yg[y] = nat[...].astype(BF)
        for i in range(1, NY):
            send(yg.at[y], yg.at[y], yg_s.at[i], yg_r.at[i], y=around(y, i, NY))

    def c_squares():
        for c in loads[8:12]:
            c.wait()
        for i in range(1, NY):
            arrived(yg.at[around(y, -i, NY)], yg_r.at[i])
        c = pltpu.make_async_copy(yg, p_out, osem.at[NZ])
        c.start()
        writes.append(c)
        whole = yg[...].reshape(R, PC).astype(F32)
        _, _, vn = moments(vmb[...], vsb[...], whole[:, 0:VC])
        _, _, on = moments(omb[...], osb[...], whole[:, VC:PC])
        row = lax.broadcasted_iota(jnp.int32, (8, 128), 0)
        st[...] = jnp.where(row < 4, jnp.sum(vn * vn), jnp.sum(on * on))
        for i in range(1, NT):
            send(st, sr.at[i], sc_s.at[i], sc_r.at[i], tp=around(t, i, NT))

    def c_scales():
        for i in range(1, NT):
            arrived(sr.at[i], sc_r.at[i])
        total = st[...]
        for i in range(1, NT):
            total = total + sr[i]
        row = lax.broadcasted_iota(jnp.int32, (8, 128), 0)
        mean = total * jnp.where(row < 4, 1.0 / (R * WIDTH), 1.0 / (R * D)).astype(F32)
        sr[0] = lax.rsqrt(mean + FLOOR)
        c = pltpu.make_async_copy(sr.at[0], s_out, osem.at[NZ + 1])
        c.start()
        writes.append(c)

    c_scatter()
    a_begin()
    b_ring(0)
    a_ring(0)
    b_ring(1)
    b_forward(0)
    c_gather()
    a_ring(1)
    b_ring(2)
    b_forward(1)
    b_end(0)
    c_project()
    a_ring(2)
    b_ring(3)
    b_forward(2)
    b_end(1)
    c_zscatter()
    a_ring(3)
    b_ring(4)
    b_forward(3)
    b_end(2)
    a_ring(4)
    b_ring(5)
    b_forward(4)
    b_end(3)
    c_zgather()
    a_ring(5)
    b_ring(6)
    b_forward(5)
    b_end(4)
    a_ring(6)
    b_ring(7)
    b_forward(6)
    b_end(5)
    c_ygather()
    a_ring(7)
    b_ring(8)
    b_forward(7)
    b_end(6)
    c_squares()
    b_forward(8)
    b_end(7)
    a_ring(8)
    b_end(8)
    c_scales()
    for c in writes:
        c.wait()
    for c in sent:
        c.wait_send()


def update_kernel(
    g_in, p_in, s_in, fv_in, fo_in, vw_in, vm_in, vs_in, ow_in, om_in, os_in,
    vstep_out, vnew_out, vcopy_out, vm_out, vs_out, ostep_out, onew_out, ocopy_out, om_out, os_out,
    gb, pbuf, sbuf, fvb, fob, vwb, vmb, vsb, owb, omb, osb,
    vstep, vnew, vcopy, ostep, onew, ocopy, fvh, foh,
    lsem, gsem, fvsem, fosem, wsem, vcsem, ocsem,
):
    z, y = lax.axis_index("z"), lax.axis_index("y")
    row = z * NY + y

    loads = []
    for k, (src, dst) in enumerate((
        (p_in, pbuf), (s_in, sbuf), (vm_in, vmb), (vs_in, vsb), (om_in, omb), (os_in, osb),
        (vw_in, vwb), (ow_in, owb),
        (fv_in.at[pl.ds(pl.multiple_of(row * VROWS, VROWS), VROWS)], fvh),
        (fo_in.at[pl.ds(pl.multiple_of(row * OROWS, OROWS), OROWS)], foh),
    )):
        c = pltpu.make_async_copy(src, dst, lsem.at[k])
        c.start()
        loads.append(c)
    fv_load = pltpu.make_async_copy(fv_in, fvb, fvsem)
    fo_load = pltpu.make_async_copy(fo_in, fob, fosem)
    fv_load.start()
    fo_load.start()
    g_loads = [pltpu.make_async_copy(g_in.at[k], gb.at[k], gsem.at[k]) for k in range(NZ)]
    for c in g_loads:
        c.start()

    for c in loads:
        c.wait()
    p = pbuf[...].reshape(R, PC).astype(F32)
    vm, vs, vn = moments(vmb[...], vsb[...], p[:, 0:VC])
    om, os, on = moments(omb[...], osb[...], p[:, VC:PC])
    vmb[...] = vm
    vsb[...] = vs
    omb[...] = om
    osb[...] = os
    writes = []

    def write(src, dst, sem):
        c = pltpu.make_async_copy(src, dst, sem)
        c.start()
        writes.append(c)

    for k, (src, dst) in enumerate(((vmb, vm_out), (vsb, vs_out), (omb, om_out), (osb, os_out))):
        write(src, dst, wsem.at[k])
    v_scale = sbuf[0:1, 0:1]
    o_scale = sbuf[4:5, 0:1]
    highest = lax.Precision.HIGHEST
    vstep[...] = v_scale * jnp.dot(fvh[...].astype(F32), vn, precision=highest, preferred_element_type=F32)
    ostep[...] = o_scale * jnp.dot(foh[...].astype(F32), on, precision=highest, preferred_element_type=F32)
    vnew[...] = vwb[...] - STEP_RATE * vstep[...]
    onew[...] = owb[...] - STEP_RATE * ostep[...]
    for k, (src, dst) in enumerate(((vstep, vstep_out), (vnew, vnew_out), (ostep, ostep_out), (onew, onew_out))):
        write(src, dst, wsem.at[4 + k])

    def two(normalized, scale):
        scaled = normalized * (scale * STEP_RATE)
        high = scaled.astype(BF)
        low = (scaled - high.astype(F32)).astype(BF)
        return jnp.concatenate([high, low], axis=0)

    v_two = two(vn, v_scale)
    o_two = two(on, o_scale)
    fv_load.wait()
    fo_load.wait()
    vt, ot = NY * VROWS, NY * OROWS
    for k in range(NZ):
        g_loads[k].wait()
        f = fvb[k * vt:(k + 1) * vt, :]
        delta = jnp.dot(jnp.concatenate([f, f], axis=1), v_two, preferred_element_type=F32)
        held = gb[k, :, 0:VROWS, :].reshape(vt, VC).astype(F32)
        vcopy[k * vt:(k + 1) * vt, :] = (held - delta).astype(BF)
        write(vcopy.at[pl.ds(k * vt, vt)], vcopy_out.at[pl.ds(k * vt, vt)], vcsem.at[k])
        f = fob[k * ot:(k + 1) * ot, :]
        delta = jnp.dot(jnp.concatenate([f, f], axis=1), o_two, preferred_element_type=F32)
        for h in range(2):
            lo = VROWS + h * OROWS
            held = gb[k, :, lo:lo + OROWS, :].reshape(ot, VC).astype(F32)
            ocopy[k * ot:(k + 1) * ot, h * VC:(h + 1) * VC] = (held - delta[:, h * VC:(h + 1) * VC]).astype(BF)
        write(ocopy.at[pl.ds(k * ot, ot)], ocopy_out.at[pl.ds(k * ot, ot)], ocsem.at[k])
    for c in writes:
        c.wait()


def per_device(
    normed_input, value_cotangent, mixer_output, output_cotangent, value_factor, output_factor,
    value_master, value_moment, value_second, output_master, output_moment, output_second,
):
    anywhere = pl.BlockSpec(memory_space=pl.ANY)
    dma = pltpu.SemaphoreType.DMA

    def vmem(shape, dtype):
        return pltpu.VMEM(shape, dtype)

    gathered, projected, scales = pl.pallas_call(
        exchange_kernel,
        name="exchange",
        out_shape=(
            jax.ShapeDtypeStruct((NZ, NY, BLK, VC), BF),
            jax.ShapeDtypeStruct((NY, R // NY, PC), BF),
            jax.ShapeDtypeStruct((8, 128), F32),
        ),
        in_specs=[anywhere] * 12,
        out_specs=(anywhere,) * 3,
        scratch_shapes=[
            vmem((TOK, FEAT), BF), vmem((TOK, VC), BF), vmem((TOK, HEAD), BF), vmem((TOK, OC), BF),
            vmem((FEAT, R), BF), vmem((HEAD, R), BF),
            vmem((VROWS, VC), F32), vmem((R, VC), F32), vmem((R, VC), F32),
            vmem((OROWS, OC), F32), vmem((R, OC), F32), vmem((R, OC), F32),
            vmem((NT, 32, TOK), BF), vmem((NT, 32, TOK), BF), vmem((NT, 32, TOK), BF),
            vmem((NY, R // NY, PC), F32), vmem((NY, R // NY, PC), BF), vmem((NY, R // NY, PC), BF),
            vmem((NZ, 16, 128), F32), vmem((NZ, 16, 128), BF), vmem((NZ, 16, 128), BF), vmem((NZ, 16, 128), BF),
            vmem((R // NY, PC), F32), vmem((NY, R // NY, PC), BF),
            vmem((8, 128), F32), vmem((NT, 8, 128), F32),
            vmem((NZ, NY, BLK, VC), BF),
            dma((12,)), dma((NZ + 2,)),
            dma((NT,)), dma((NT,)), dma((NT,)), dma((NT,)), dma((NT,)), dma((NT,)),
            dma((NY,)), dma((NY,)), dma((NY,)), dma((NY,)),
            dma((NZ,)), dma((NZ,)), dma((NZ,)), dma((NZ,)),
            dma((NY,)), dma((NY,)),
            dma((2, NZ // 2 + 1)), dma((2, NZ // 2 + 1)), dma((2, NZ // 2 + 1)), dma((2, NZ // 2 + 1)),
            dma((4, NZ)), dma((4, NZ)),
        ],
        compiler_params=pltpu.CompilerParams(collective_id=0, has_side_effects=True),
    )(
        normed_input, value_cotangent, mixer_output, output_cotangent, value_factor, output_factor,
        value_master, value_moment, value_second, output_master, output_moment, output_second,
    )

    def like(a, dtype=F32):
        return jax.ShapeDtypeStruct(a, dtype)

    return pl.pallas_call(
        update_kernel,
        name="update",
        out_shape=(
            like((VROWS, VC)), like((VROWS, VC)), like((D, VC), BF), like((R, VC)), like((R, VC)),
            like((OROWS, OC)), like((OROWS, OC)), like((WIDTH, OC), BF), like((R, OC)), like((R, OC)),
        ),
        in_specs=[anywhere] * 11,
        out_specs=(anywhere,) * 10,
        scratch_shapes=[
            vmem((NZ, NY, BLK, VC), BF), vmem((NY, R // NY, PC), BF), vmem((8, 128), F32),
            vmem((D, R), BF), vmem((WIDTH, R), BF),
            vmem((VROWS, VC), F32), vmem((R, VC), F32), vmem((R, VC), F32),
            vmem((OROWS, OC), F32), vmem((R, OC), F32), vmem((R, OC), F32),
            vmem((VROWS, VC), F32), vmem((VROWS, VC), F32), vmem((D, VC), BF),
            vmem((OROWS, OC), F32), vmem((OROWS, OC), F32), vmem((WIDTH, OC), BF),
            vmem((VROWS, R), BF), vmem((OROWS, R), BF),
            dma((10,)), dma((NZ,)), dma, dma, dma((8,)), dma((NZ,)), dma((NZ,)),
        ],
    )(
        gathered, projected, scales, value_factor, output_factor,
        value_master, value_moment, value_second, output_master, output_moment, output_second,
    )


def solution(mesh):
    finer = Mesh(mesh.devices.reshape(NZ, NY, NT), ("z", "y", "tp"))
    fs = ("z", "y")
    rows, cols = P(fs, "tp"), P(None, "tp")
    return jax.shard_map(
        per_device,
        mesh=finer,
        in_specs=(rows, rows, rows, rows, P(), P(), rows, cols, cols, rows, cols, cols),
        out_specs=(rows, rows, cols, cols, cols, rows, rows, cols, cols, cols),
        check_vma=False,
    )
```

```python
import jax
import jax.numpy as jnp
from jax import lax
from jax.experimental import pallas as pl
from jax.experimental.pallas import tpu as pltpu
from jax.sharding import Mesh
from jax.sharding import PartitionSpec as P

D = 4096
WIDTH = 2048
R = 128
TOK = 512
NZ, NY, NT = 16, 4, 8
FEAT = D // NT
HEAD = WIDTH // NT
VC = WIDTH // NT
OC = D // NT
PC = VC + OC
VROWS = D // (NZ * NY)
OROWS = WIDTH // (NZ * NY)
BLK = VROWS + 2 * OROWS
ASPLIT = 48
BHALF = 96

BETA_ONE = 0.8
BETA_TWO = 0.9
EPSILON = 1e-08
STEP_RATE = 0.005
FLOOR = 0.25

BF = jnp.bfloat16
F32 = jnp.float32
MESH = pl.DeviceIdType.MESH


def moments(first, second, projected):
    first_new = BETA_ONE * first + (1.0 - BETA_ONE) * projected
    second_new = BETA_TWO * second + (1.0 - BETA_TWO) * projected * projected
    normalized = first_new / (jnp.sqrt(second_new) + EPSILON)
    return first_new, second_new, normalized


def exchange_kernel(
    n_in, vc_in, mo_in, oc_in, fv_in, fo_in, vw_in, vm_in, vs_in, ow_in, om_in, os_in,
    g, scales, vn_out, on_out, vmb, vsb, omb, osb, fv_all, fo_all, vwb, owb,
    nb, vcb, mob, ocb, fvb, fob,
    xs, xr, xg, pfv, pfo, pbv, pbo, yrv, yro, zs, zb, zr, zg, nat, yg, st, sr, sy, syr,
    lsem, tok,
    xs_s, xs_r, xg_s, xg_r, sc_s, sc_r, sy_s, sy_r, yr_s, yr_r, yg_s, yg_r,
    zr_s, zr_r, zg_s, zg_r, ay_s, ay_r, az_s, az_r, bz_s, bz_r, by_s, by_r,
):
    z, y, t = lax.axis_index("z"), lax.axis_index("y"), lax.axis_index("tp")

    def around(k, i, n):
        return lax.rem(k + (i + n), n)

    up, down = around(z, 1, NZ), around(z, -1, NZ)
    yup, ydown = around(y, 1, NY), around(y, -1, NY)

    barrier = pltpu.get_barrier_semaphore()
    for i in range(1, NT):
        pl.semaphore_signal(barrier, inc=1, device_id={"tp": around(t, i, NT)}, device_id_type=MESH)
    for i in range(1, NY):
        pl.semaphore_signal(barrier, inc=1, device_id={"y": around(y, i, NY)}, device_id_type=MESH)
    for k in (up, down):
        pl.semaphore_signal(barrier, inc=1, device_id={"z": k}, device_id_type=MESH)

    loads = []
    for k, (src, dst) in enumerate((
        (fo_in.at[pl.ds(pl.multiple_of(t * HEAD, HEAD), HEAD)], fob), (mo_in, mob),
        (fv_in.at[pl.ds(pl.multiple_of(t * FEAT, FEAT), FEAT)], fvb), (n_in, nb),
        (vw_in, vwb), (ow_in, owb),
        (oc_in, ocb), (vc_in, vcb),
        (vm_in, vmb), (vs_in, vsb), (om_in, omb), (os_in, osb),
        (fv_in, fv_all), (fo_in, fo_all),
    )):
        c = pltpu.make_async_copy(src, dst, lsem.at[k])
        c.start()
        loads.append(c)

    sent = []

    def remote(src, dst, ssem, rsem, **where):
        return pltpu.make_async_remote_copy(
            src_ref=src, dst_ref=dst, send_sem=ssem, recv_sem=rsem,
            device_id=where, device_id_type=MESH,
        )

    def send(src, dst, ssem, rsem, **where):
        c = remote(src, dst, ssem, rsem, **where)
        c.start()
        sent.append(c)

    def arrived(dst, rsem):
        remote(dst, dst, rsem, rsem, tp=t).wait_recv()

    def a_rows(k, ys=None):
        return g.at[k, :, pl.ds(0, ASPLIT), :] if ys is None else g.at[k, pl.ds(ys, NY // 2), pl.ds(0, ASPLIT), :]

    def b_rows(k, j=None, part=None):
        lo, hi = {None: (ASPLIT, BLK), 0: (ASPLIT, BHALF), 1: (BHALF, BLK)}[part]
        return g.at[k, y if j is None else j, pl.ds(lo, hi - lo), :]

    LAST = NZ // 2

    def a_begin():
        own = g.at[z, y, pl.ds(0, ASPLIT), :]
        for i in range(1, NY):
            send(own, own, ay_s.at[i], ay_r.at[i], y=around(y, i, NY))

    def a_ring(s):
        if s == 0:
            for i in range(1, NY):
                arrived(g.at[z, around(y, -i, NY), pl.ds(0, ASPLIT), :], ay_r.at[i])
        below, above = around(z, -s, NZ), around(z, s, NZ)
        if 0 < s < LAST:
            arrived(a_rows(below), az_r.at[0, s])
            arrived(a_rows(above), az_r.at[1, s])
        if s == LAST:
            arrived(a_rows(below, 0), az_r.at[0, s])
            arrived(a_rows(above, NY // 2), az_r.at[1, s])
            return
        half = s + 1 == LAST
        for d, (k, to) in enumerate(((below, up), (above, down))):
            block = a_rows(k, d * (NY // 2)) if half else a_rows(k)
            send(block, block, az_s.at[d, s + 1], az_r.at[d, s + 1], z=to)

    def b_across(k, b):
        block = b_rows(k)
        send(block, block, by_s.at[0, b], by_r.at[0, b], y=yup)
        send(block, block, by_s.at[1, b], by_r.at[1, b], y=ydown)

    def b_ids(s):
        if s == 0:
            return ((0, 0),)
        if s == LAST:
            return ((LAST, NZ - 1),)
        return ((-s, 2 * s - 1), (s, 2 * s))

    def b_ring(s):
        below, above = around(z, -s, NZ), around(z, s, NZ)
        if 0 < s < LAST:
            arrived(b_rows(below), bz_r.at[0, s])
            arrived(b_rows(above), bz_r.at[1, s])
        if s == LAST:
            arrived(b_rows(below, part=0), bz_r.at[0, s])
            arrived(b_rows(above, part=1), bz_r.at[1, s])
        else:
            half = s + 1 == LAST
            for d, (k, to) in enumerate(((below, up), (above, down))):
                block = b_rows(k, part=d) if half else b_rows(k)
                send(block, block, bz_s.at[d, s + 1], bz_r.at[d, s + 1], z=to)
        for off, b in b_ids(s):
            b_across(around(z, off, NZ), b)

    def b_forward(s):
        for off, b in b_ids(s):
            k = around(z, off, NZ)
            arrived(b_rows(k, ydown), by_r.at[0, b])
            block = b_rows(k, ydown, 0)
            send(block, block, by_s.at[2, b], by_r.at[2, b], y=yup)
            arrived(b_rows(k, yup), by_r.at[1, b])
            block = b_rows(k, yup, 1)
            send(block, block, by_s.at[3, b], by_r.at[3, b], y=ydown)

    def b_end(s):
        across = around(y, 2, NY)
        for off, b in b_ids(s):
            k = around(z, off, NZ)
            arrived(b_rows(k, across, 0), by_r.at[2, b])
            arrived(b_rows(k, across, 1), by_r.at[3, b])

    def token():
        pl.semaphore_signal(tok.at[0], inc=1, device_id={"z": up}, device_id_type=MESH)
        pl.semaphore_signal(tok.at[1], inc=1, device_id={"z": down}, device_id_type=MESH)
        pl.semaphore_wait(tok.at[0], 1)
        pl.semaphore_wait(tok.at[1], 1)

    nt = (((1,), (1,)), ((), ()))

    def c_partial(w):
        for c in loads[2 - 2 * w:4 - 2 * w]:
            c.wait()
        factor, rows = (fob, mob) if w else (fvb, nb)
        part = lax.dot_general(factor[...].T, rows[...], nt, preferred_element_type=F32)
        xs[w] = part.astype(BF).reshape(NT, 16, TOK)

    def c_scatter(w):
        for i in range(1, NT):
            to = around(t, i, NT)
            send(xs.at[w, to], xr.at[w, i], xs_s.at[w, i], xs_r.at[w, i], tp=to)

    def c_gather(w):
        for i in range(1, NT):
            arrived(xr.at[w, i], xs_r.at[w, i])
        total = xs[w, t].astype(F32)
        for i in range(1, NT):
            total = total + xr[w, i].astype(F32)
        xg[w, t] = total.astype(BF)
        for i in range(1, NT):
            send(xg.at[w, t], xg.at[w, t], xg_s.at[w, i], xg_r.at[w, i], tp=around(t, i, NT))

    def c_project(w):
        loads[7 - w].wait()
        for i in range(1, NT):
            arrived(xg.at[w, around(t, -i, NT)], xg_r.at[w, i])
        right, whole, rounded, landing = (ocb, pfo, pbo, yro) if w else (vcb, pfv, pbv, yrv)
        p = jnp.dot(xg[w].reshape(R, TOK), right[...], preferred_element_type=F32)
        p = p.reshape(NY, R // NY, p.shape[-1])
        whole[...] = p
        rounded[...] = p.astype(BF)
        for i in range(1, NY):
            to = around(y, i, NY)
            send(rounded.at[to], landing.at[i], yr_s.at[w, i], yr_r.at[w, i], y=to)

    def c_zscatter():
        for i in range(1, NY):
            arrived(yro.at[i], yr_r.at[1, i])
        total = pfo[y]
        for i in range(1, NY):
            total = total + yro[i].astype(F32)
        for k in range(NZ):
            q, r = divmod(k, 4)
            zs[k, 0:8, :] = total[8 * q:8 * q + 8, 128 * r:128 * r + 128]
        for i in range(1, NY):
            arrived(yrv.at[i], yr_r.at[0, i])
        total = pfv[y]
        for i in range(1, NY):
            total = total + yrv[i].astype(F32)
        for k in range(NZ):
            q, r = divmod(k, 2)
            zs[k, 8:12, :] = total[4 * q:4 * q + 4, 128 * r:128 * r + 128]
            zs[k, 12:16, :] = jnp.zeros((4, 128), F32)
        zb[...] = zs[...].astype(BF)
        for i in range(1, NZ):
            to = around(z, i, NZ)
            send(zb.at[to], zr.at[i], zr_s.at[i], zr_r.at[i], z=to)

    def c_zgather():
        for c in loads[8:12]:
            c.wait()
        down8 = pl.multiple_of(y * (R // NY) + 8 * (z // 4), 8)
        o_cols = pl.ds(pl.multiple_of(128 * lax.rem(z, 4), 128), 128)
        v_cols = pl.ds(pl.multiple_of(128 * lax.rem(z, 2), 128), 128)
        rows8 = pl.ds(down8, 8)
        om, osq = omb[rows8, o_cols], osb[rows8, o_cols]
        vm, vsq = vmb[rows8, v_cols], vsb[rows8, v_cols]
        second = lax.rem(z // 2, 2) == 1
        vm = jnp.where(second, vm[4:8], vm[0:4])
        vsq = jnp.where(second, vsq[4:8], vsq[0:4])
        for i in range(1, NZ):
            arrived(zr.at[i], zr_r.at[i])
        total = zs[z]
        for i in range(1, NZ):
            total = total + zr[i].astype(F32)
        held = total.astype(BF).astype(F32)
        _, _, on = moments(om, osq, held[0:8])
        _, _, vn = moments(vm, vsq, held[8:12])
        o_sum = jnp.sum(on * on, axis=0, keepdims=True)
        v_sum = jnp.sum(vn * vn, axis=0, keepdims=True)
        o_high, v_high = o_sum.astype(BF).astype(F32), v_sum.astype(BF).astype(F32)
        row = lax.broadcasted_iota(jnp.int32, (16, 128), 0)
        for k, line in enumerate((v_high, v_sum - v_high, o_high, o_sum - o_high)):
            total = jnp.where(row == 12 + k, line, total)
        zg[z] = total.astype(BF)
        for i in range(1, NZ):
            send(zg.at[z], zg.at[z], zg_s.at[i], zg_r.at[i], z=around(z, i, NZ))

    def c_ygather():
        for i in range(1, NZ):
            arrived(zg.at[around(z, -i, NZ)], zg_r.at[i])
        lines = jnp.zeros((4, 128), F32)
        for k in range(NZ):
            chunk = zg[k].astype(F32)
            q, r = divmod(k, 4)
            nat[8 * q:8 * q + 8, VC + 128 * r:VC + 128 * r + 128] = chunk[0:8]
            q, r = divmod(k, 2)
            nat[4 * q:4 * q + 4, 128 * r:128 * r + 128] = chunk[8:12]
            lines = lines + chunk[12:16]
        yg[y] = nat[...].astype(BF)
        for i in range(1, NY):
            send(yg.at[y], yg.at[y], yg_s.at[i], yg_r.at[i], y=around(y, i, NY))
        row = lax.broadcasted_iota(jnp.int32, (8, 128), 0)
        st[...] = jnp.where(row < 4, lines[0:1] + lines[1:2], lines[2:3] + lines[3:4])
        for i in range(1, NT):
            send(st, sr.at[i], sc_s.at[i], sc_r.at[i], tp=around(t, i, NT))

    def c_squares():
        for i in range(1, NT):
            arrived(sr.at[i], sc_r.at[i])
        total = st[...]
        for i in range(1, NT):
            total = total + sr[i]
        sy[...] = total
        for i in range(1, NY):
            send(sy, syr.at[i], sy_s.at[i], sy_r.at[i], y=around(y, i, NY))

    def c_moments():
        for i in range(1, NY):
            arrived(yg.at[around(y, -i, NY)], yg_r.at[i])
        whole = yg[...].reshape(R, PC).astype(F32)
        vmb[...], vsb[...], vn_out[...] = moments(vmb[...], vsb[...], whole[:, 0:VC])
        omb[...], osb[...], on_out[...] = moments(omb[...], osb[...], whole[:, VC:PC])

    def c_scales():
        for i in range(1, NY):
            arrived(syr.at[i], sy_r.at[i])
        total = sy[...]
        for i in range(1, NY):
            total = total + syr[i]
        row = lax.broadcasted_iota(jnp.int32, (8, 128), 0)
        mean = jnp.sum(total, axis=1, keepdims=True) * jnp.where(row < 4, 1.0 / (R * WIDTH), 1.0 / (R * D))
        scales[...] = lax.rsqrt(mean + FLOOR)

    c_partial(1)
    pl.semaphore_wait(barrier, NT + NY)
    c_scatter(1)
    c_partial(0)
    c_scatter(0)
    for c in loads[4:6]:
        c.wait()
    g[z, y, 0:VROWS, :] = vwb[...].astype(BF)
    g[z, y, VROWS:VROWS + OROWS, :] = owb[:, 0:VC].astype(BF)
    g[z, y, VROWS + OROWS:BLK, :] = owb[:, VC:OC].astype(BF)
    a_begin()
    b_ring(0)
    token()
    token()
    c_gather(1)
    token()
    a_ring(0)
    c_gather(0)
    token()
    token()
    b_ring(1)
    b_forward(0)
    c_project(1)
    c_project(0)
    token()
    token()
    a_ring(1)
    b_ring(2)
    b_forward(1)
    c_zscatter()
    a_ring(2)
    b_ring(3)
    b_forward(2)
    a_ring(3)
    b_ring(4)
    b_forward(3)
    c_zgather()
    a_ring(4)
    b_ring(5)
    b_forward(4)
    a_ring(5)
    b_ring(6)
    b_forward(5)
    c_ygather()
    a_ring(6)
    b_ring(7)
    b_forward(6)
    c_squares()
    a_ring(7)
    b_ring(8)
    b_forward(7)
    c_moments()
    b_forward(8)
    c_scales()
    a_ring(8)
    for s in range(LAST + 1):
        b_end(s)
    for c in loads[12:]:
        c.wait()
    for c in sent:
        c.wait_send()


def update_kernel(
    g, scales, vn, on, vm, vs, om, os, fv, fo, vw, ow,
    vstep_out, vnew_out, vcopy_out, vm_out, vs_out, ostep_out, onew_out, ocopy_out, om_out, os_out,
    vstep, vnew, vcopy, ostep, onew, ocopy, wsem, vcsem, ocsem,
):
    z, y = lax.axis_index("z"), lax.axis_index("y")
    row = z * NY + y
    writes = []

    def write(src, dst, sem):
        c = pltpu.make_async_copy(src, dst, sem)
        c.start()
        writes.append(c)

    for k, (src, dst) in enumerate(((vm, vm_out), (vs, vs_out), (om, om_out), (os, os_out))):
        write(src, dst, wsem.at[k])
    v_scale = scales[0:1, 0:1]
    o_scale = scales[4:5, 0:1]

    def two(normalized, scale):
        scaled = normalized * (scale * STEP_RATE)
        high = scaled.astype(BF)
        low = (scaled - high.astype(F32)).astype(BF)
        return jnp.concatenate([high, low], axis=0)

    v_two = two(vn[...], v_scale)
    o_two = two(on[...], o_scale)
    vt, ot = NY * VROWS, NY * OROWS
    for k in range(NZ):
        f = fv[k * vt:(k + 1) * vt, :]
        delta = jnp.dot(jnp.concatenate([f, f], axis=1), v_two, preferred_element_type=F32)
        held = g[k, :, 0:VROWS, :].reshape(vt, VC).astype(F32)
        vcopy[k * vt:(k + 1) * vt, :] = (held - delta).astype(BF)
        write(vcopy.at[pl.ds(k * vt, vt)], vcopy_out.at[pl.ds(k * vt, vt)], vcsem.at[k])
        f = fo[k * ot:(k + 1) * ot, :]
        delta = jnp.dot(jnp.concatenate([f, f], axis=1), o_two, preferred_element_type=F32)
        for h in range(2):
            lo = VROWS + h * OROWS
            held = g[k, :, lo:lo + OROWS, :].reshape(ot, VC).astype(F32)
            ocopy[k * ot:(k + 1) * ot, h * VC:(h + 1) * VC] = (held - delta[:, h * VC:(h + 1) * VC]).astype(BF)
        write(ocopy.at[pl.ds(k * ot, ot)], ocopy_out.at[pl.ds(k * ot, ot)], ocsem.at[k])
    highest = lax.Precision.HIGHEST
    v_here = fv[pl.ds(pl.multiple_of(row * VROWS, VROWS), VROWS), :].astype(F32)
    o_here = fo[pl.ds(pl.multiple_of(row * OROWS, OROWS), OROWS), :].astype(F32)
    vstep[...] = v_scale * jnp.dot(v_here, vn[...], precision=highest, preferred_element_type=F32)
    ostep[...] = o_scale * jnp.dot(o_here, on[...], precision=highest, preferred_element_type=F32)
    vnew[...] = vw[...] - STEP_RATE * vstep[...]
    onew[...] = ow[...] - STEP_RATE * ostep[...]
    for k, (src, dst) in enumerate(((vstep, vstep_out), (vnew, vnew_out), (ostep, ostep_out), (onew, onew_out))):
        write(src, dst, wsem.at[4 + k])
    for c in writes:
        c.wait()


def per_device(
    normed_input, value_cotangent, mixer_output, output_cotangent, value_factor, output_factor,
    value_master, value_moment, value_second, output_master, output_moment, output_second,
):
    anywhere = pl.BlockSpec(memory_space=pl.ANY)
    inside = pl.BlockSpec(memory_space=pltpu.VMEM)
    dma = pltpu.SemaphoreType.DMA

    def vmem(shape, dtype):
        return pltpu.VMEM(shape, dtype)

    handed = (
        vmem((NZ, NY, BLK, VC), BF), vmem((8, 128), F32), vmem((R, VC), F32), vmem((R, OC), F32),
        vmem((R, VC), F32), vmem((R, VC), F32), vmem((R, OC), F32), vmem((R, OC), F32),
        vmem((D, R), BF), vmem((WIDTH, R), BF), vmem((VROWS, VC), F32), vmem((OROWS, OC), F32),
    )
    state = pl.pallas_call(
        exchange_kernel,
        name="exchange",
        out_shape=handed,
        in_specs=[anywhere] * 12,
        out_specs=(inside,) * len(handed),
        scratch_shapes=[
            vmem((TOK, FEAT), BF), vmem((TOK, VC), BF), vmem((TOK, HEAD), BF), vmem((TOK, OC), BF),
            vmem((FEAT, R), BF), vmem((HEAD, R), BF),
            vmem((2, NT, 16, TOK), BF), vmem((2, NT, 16, TOK), BF), vmem((2, NT, 16, TOK), BF),
            vmem((NY, R // NY, VC), F32), vmem((NY, R // NY, OC), F32),
            vmem((NY, R // NY, VC), BF), vmem((NY, R // NY, OC), BF),
            vmem((NY, R // NY, VC), BF), vmem((NY, R // NY, OC), BF),
            vmem((NZ, 16, 128), F32), vmem((NZ, 16, 128), BF), vmem((NZ, 16, 128), BF), vmem((NZ, 16, 128), BF),
            vmem((R // NY, PC), F32), vmem((NY, R // NY, PC), BF),
            vmem((8, 128), F32), vmem((NT, 8, 128), F32), vmem((8, 128), F32), vmem((NY, 8, 128), F32),
            dma((14,)), pltpu.SemaphoreType.REGULAR((2,)),
            dma((2, NT)), dma((2, NT)), dma((2, NT)), dma((2, NT)), dma((NT,)), dma((NT,)), dma((NY,)), dma((NY,)),
            dma((2, NY)), dma((2, NY)), dma((NY,)), dma((NY,)),
            dma((NZ,)), dma((NZ,)), dma((NZ,)), dma((NZ,)),
            dma((NY,)), dma((NY,)),
            dma((2, NZ // 2 + 1)), dma((2, NZ // 2 + 1)), dma((2, NZ // 2 + 1)), dma((2, NZ // 2 + 1)),
            dma((4, NZ)), dma((4, NZ)),
        ],
        compiler_params=pltpu.CompilerParams(collective_id=0, has_side_effects=True, vmem_limit_bytes=30 << 20),
    )(
        normed_input, value_cotangent, mixer_output, output_cotangent, value_factor, output_factor,
        value_master, value_moment, value_second, output_master, output_moment, output_second,
    )

    def like(a, dtype=F32):
        return jax.ShapeDtypeStruct(a, dtype)

    return pl.pallas_call(
        update_kernel,
        name="update",
        out_shape=(
            like((VROWS, VC)), like((VROWS, VC)), like((D, VC), BF), like((R, VC)), like((R, VC)),
            like((OROWS, OC)), like((OROWS, OC)), like((WIDTH, OC), BF), like((R, OC)), like((R, OC)),
        ),
        in_specs=[inside] * len(handed),
        out_specs=(anywhere,) * 10,
        scratch_shapes=[
            vmem((VROWS, VC), F32), vmem((VROWS, VC), F32), vmem((D, VC), BF),
            vmem((OROWS, OC), F32), vmem((OROWS, OC), F32), vmem((WIDTH, OC), BF),
            dma((8,)), dma((NZ,)), dma((NZ,)),
        ],
        compiler_params=pltpu.CompilerParams(vmem_limit_bytes=30 << 20),
    )(*state)


def solution(mesh):
    finer = Mesh(mesh.devices.reshape(NZ, NY, NT), ("z", "y", "tp"))
    fs = ("z", "y")
    rows, cols = P(fs, "tp"), P(None, "tp")
    return jax.shard_map(
        per_device,
        mesh=finer,
        in_specs=(rows, rows, rows, rows, P(), P(), rows, cols, cols, rows, cols, cols),
        out_specs=(rows, rows, cols, cols, cols, rows, rows, cols, cols, cols),
        check_vma=False,
    )
```

```python
import jax
import jax.numpy as jnp
from jax import lax
from jax.experimental import pallas as pl
from jax.experimental.pallas import tpu as pltpu
from jax.sharding import Mesh
from jax.sharding import PartitionSpec as P

D = 4096
WIDTH = 2048
R = 128
TOK = 512
NZ, NY, NT = 16, 4, 8
FEAT = D // NT
HEAD = WIDTH // NT
VC = WIDTH // NT
OC = D // NT
PC = VC + OC
VROWS = D // (NZ * NY)
OROWS = WIDTH // (NZ * NY)
BLK = VROWS + 2 * OROWS
ASPLIT = 16
BHALF = 64

BETA_ONE = 0.8
BETA_TWO = 0.9
EPSILON = 1e-08
STEP_RATE = 0.005
FLOOR = 0.25

BF = jnp.bfloat16
F32 = jnp.float32
MESH = pl.DeviceIdType.MESH


def moments(first, second, projected):
    first_new = BETA_ONE * first + (1.0 - BETA_ONE) * projected
    second_new = BETA_TWO * second + (1.0 - BETA_TWO) * projected * projected
    normalized = first_new / (jnp.sqrt(second_new) + EPSILON)
    return first_new, second_new, normalized


def exchange_kernel(
    n_in, vc_in, mo_in, oc_in, fv_in, fo_in, vw_in, vm_in, vs_in, ow_in, om_in, os_in,
    g, scales, vn_out, on_out, vmb, vsb, omb, osb, fv_all, fo_all, vwb, owb,
    nb, vcb, mob, ocb, fvb, fob,
    xs, xr, xg, pfv, pfo, pbv, pbo, yrv, yro, zs, zb, zr, zg, nat, yg, st, sr, sy, syr,
    lsem, tok,
    xs_s, xs_r, xg_s, xg_r, sc_s, sc_r, sy_s, sy_r, yr_s, yr_r, yg_s, yg_r,
    zr_s, zr_r, zg_s, zg_r, ay_s, ay_r, az_s, az_r, bz_s, bz_r, by_s, by_r,
):
    z, y, t = lax.axis_index("z"), lax.axis_index("y"), lax.axis_index("tp")

    def around(k, i, n):
        return lax.rem(k + (i + n), n)

    up, down = around(z, 1, NZ), around(z, -1, NZ)
    yup, ydown = around(y, 1, NY), around(y, -1, NY)

    barrier = pltpu.get_barrier_semaphore()
    for i in range(1, NT):
        pl.semaphore_signal(barrier, inc=1, device_id={"tp": around(t, i, NT)}, device_id_type=MESH)
    for i in range(1, NY):
        pl.semaphore_signal(barrier, inc=1, device_id={"y": around(y, i, NY)}, device_id_type=MESH)
    for k in (up, down):
        pl.semaphore_signal(barrier, inc=1, device_id={"z": k}, device_id_type=MESH)

    loads = []
    for k, (src, dst) in enumerate((
        (vw_in, vwb), (ow_in, owb),
        (fo_in.at[pl.ds(pl.multiple_of(t * HEAD, HEAD), HEAD)], fob), (mo_in, mob),
        (fv_in.at[pl.ds(pl.multiple_of(t * FEAT, FEAT), FEAT)], fvb), (n_in, nb),
        (oc_in, ocb), (vc_in, vcb),
        (vm_in, vmb), (vs_in, vsb), (om_in, omb), (os_in, osb),
        (fv_in, fv_all), (fo_in, fo_all),
    )):
        c = pltpu.make_async_copy(src, dst, lsem.at[k])
        c.start()
        loads.append(c)

    sent = []

    def remote(src, dst, ssem, rsem, **where):
        return pltpu.make_async_remote_copy(
            src_ref=src, dst_ref=dst, send_sem=ssem, recv_sem=rsem,
            device_id=where, device_id_type=MESH,
        )

    def send(src, dst, ssem, rsem, **where):
        c = remote(src, dst, ssem, rsem, **where)
        c.start()
        sent.append(c)

    def arrived(dst, rsem):
        remote(dst, dst, rsem, rsem, tp=t).wait_recv()

    def a_rows(k, h):
        return g.at[k, pl.ds(h * (NY // 2), NY // 2), pl.ds(0, ASPLIT), :]

    def b_rows(k, j=None, part=None):
        lo, hi = {None: (ASPLIT, BLK), 0: (ASPLIT, BHALF), 1: (BHALF, BLK)}[part]
        return g.at[k, y if j is None else j, pl.ds(lo, hi - lo), :]

    LAST = NZ // 2

    def a_begin():
        own = g.at[z, y, pl.ds(0, ASPLIT), :]
        for i in range(1, NY):
            send(own, own, ay_s.at[i], ay_r.at[i], y=around(y, i, NY))

    def a_ring(s, h):
        if s == 0 and h == 0:
            for i in range(1, NY):
                arrived(g.at[z, around(y, -i, NY), pl.ds(0, ASPLIT), :], ay_r.at[i])
        for d, (k, to) in enumerate(((around(z, -s, NZ), up), (around(z, s, NZ), down))):
            if 0 < s < LAST or (s == LAST and d == h):
                arrived(a_rows(k, h), az_r.at[d, h, s])
            if s + 1 < LAST or (s + 1 == LAST and d == h):
                send(a_rows(k, h), a_rows(k, h), az_s.at[d, h, s + 1], az_r.at[d, h, s + 1], z=to)

    def b_across(k, b):
        block = b_rows(k)
        send(block, block, by_s.at[0, b], by_r.at[0, b], y=yup)
        send(block, block, by_s.at[1, b], by_r.at[1, b], y=ydown)

    def b_ids(s):
        if s == 0:
            return ((0, 0),)
        if s == LAST:
            return ((LAST, NZ - 1),)
        return ((-s, 2 * s - 1), (s, 2 * s))

    def b_ring(s):
        below, above = around(z, -s, NZ), around(z, s, NZ)
        if 0 < s < LAST:
            arrived(b_rows(below), bz_r.at[0, s])
            arrived(b_rows(above), bz_r.at[1, s])
        if s == LAST:
            arrived(b_rows(below, part=0), bz_r.at[0, s])
            arrived(b_rows(above, part=1), bz_r.at[1, s])
        else:
            half = s + 1 == LAST
            for d, (k, to) in enumerate(((below, up), (above, down))):
                block = b_rows(k, part=d) if half else b_rows(k)
                send(block, block, bz_s.at[d, s + 1], bz_r.at[d, s + 1], z=to)
        for off, b in b_ids(s):
            b_across(around(z, off, NZ), b)

    def b_forward(s):
        for off, b in b_ids(s):
            k = around(z, off, NZ)
            arrived(b_rows(k, ydown), by_r.at[0, b])
            block = b_rows(k, ydown, 0)
            send(block, block, by_s.at[2, b], by_r.at[2, b], y=yup)
            arrived(b_rows(k, yup), by_r.at[1, b])
            block = b_rows(k, yup, 1)
            send(block, block, by_s.at[3, b], by_r.at[3, b], y=ydown)

    def b_end(s):
        across = around(y, 2, NY)
        for off, b in b_ids(s):
            k = around(z, off, NZ)
            arrived(b_rows(k, across, 0), by_r.at[2, b])
            arrived(b_rows(k, across, 1), by_r.at[3, b])

    def token():
        pl.semaphore_signal(tok.at[0], inc=1, device_id={"z": up}, device_id_type=MESH)
        pl.semaphore_signal(tok.at[1], inc=1, device_id={"z": down}, device_id_type=MESH)
        pl.semaphore_wait(tok.at[0], 1)
        pl.semaphore_wait(tok.at[1], 1)

    nt = (((1,), (1,)), ((), ()))

    def c_partial(w):
        for c in loads[4 - 2 * w:6 - 2 * w]:
            c.wait()
        factor, rows = (fob, mob) if w else (fvb, nb)
        part = lax.dot_general(factor[...].T, rows[...], nt, preferred_element_type=F32)
        xs[w] = part.astype(BF).reshape(NT, 16, TOK)

    def c_scatter(w):
        for i in range(1, NT):
            to = around(t, i, NT)
            send(xs.at[w, to], xr.at[w, i], xs_s.at[w, i], xs_r.at[w, i], tp=to)

    def c_gather(w):
        for i in range(1, NT):
            arrived(xr.at[w, i], xs_r.at[w, i])
        total = xs[w, t].astype(F32)
        for i in range(1, NT):
            total = total + xr[w, i].astype(F32)
        xg[w, t] = total.astype(BF)
        for i in range(1, NT):
            send(xg.at[w, t], xg.at[w, t], xg_s.at[w, i], xg_r.at[w, i], tp=around(t, i, NT))

    def c_project(w):
        loads[7 - w].wait()
        for i in range(1, NT):
            arrived(xg.at[w, around(t, -i, NT)], xg_r.at[w, i])
        right, whole, rounded, landing = (ocb, pfo, pbo, yro) if w else (vcb, pfv, pbv, yrv)
        p = jnp.dot(xg[w].reshape(R, TOK), right[...], preferred_element_type=F32)
        p = p.reshape(NY, R // NY, p.shape[-1])
        whole[...] = p
        rounded[...] = p.astype(BF)
        for i in range(1, NY):
            to = around(y, i, NY)
            send(rounded.at[to], landing.at[i], yr_s.at[w, i], yr_r.at[w, i], y=to)

    def c_zscatter():
        for i in range(1, NY):
            arrived(yro.at[i], yr_r.at[1, i])
        total = pfo[y]
        for i in range(1, NY):
            total = total + yro[i].astype(F32)
        for k in range(NZ):
            q, r = divmod(k, 4)
            zs[k, 0:8, :] = total[8 * q:8 * q + 8, 128 * r:128 * r + 128]
        for i in range(1, NY):
            arrived(yrv.at[i], yr_r.at[0, i])
        total = pfv[y]
        for i in range(1, NY):
            total = total + yrv[i].astype(F32)
        for k in range(NZ):
            q, r = divmod(k, 2)
            zs[k, 8:12, :] = total[4 * q:4 * q + 4, 128 * r:128 * r + 128]
            zs[k, 12:16, :] = jnp.zeros((4, 128), F32)
        zb[...] = zs[...].astype(BF)
        for i in range(1, NZ):
            to = around(z, i, NZ)
            send(zb.at[to], zr.at[i], zr_s.at[i], zr_r.at[i], z=to)

    def c_zgather():
        for c in loads[8:12]:
            c.wait()
        down8 = pl.multiple_of(y * (R // NY) + 8 * (z // 4), 8)
        o_cols = pl.ds(pl.multiple_of(128 * lax.rem(z, 4), 128), 128)
        v_cols = pl.ds(pl.multiple_of(128 * lax.rem(z, 2), 128), 128)
        rows8 = pl.ds(down8, 8)
        om, osq = omb[rows8, o_cols], osb[rows8, o_cols]
        vm, vsq = vmb[rows8, v_cols], vsb[rows8, v_cols]
        second = lax.rem(z // 2, 2) == 1
        vm = jnp.where(second, vm[4:8], vm[0:4])
        vsq = jnp.where(second, vsq[4:8], vsq[0:4])
        for i in range(1, NZ):
            arrived(zr.at[i], zr_r.at[i])
        total = zs[z]
        for i in range(1, NZ):
            total = total + zr[i].astype(F32)
        held = total.astype(BF).astype(F32)
        _, _, on = moments(om, osq, held[0:8])
        _, _, vn = moments(vm, vsq, held[8:12])
        o_sum = jnp.sum(on * on, axis=0, keepdims=True)
        v_sum = jnp.sum(vn * vn, axis=0, keepdims=True)
        o_high, v_high = o_sum.astype(BF).astype(F32), v_sum.astype(BF).astype(F32)
        row = lax.broadcasted_iota(jnp.int32, (16, 128), 0)
        for k, line in enumerate((v_high, v_sum - v_high, o_high, o_sum - o_high)):
            total = jnp.where(row == 12 + k, line, total)
        zg[z] = total.astype(BF)
        for i in range(1, NZ):
            send(zg.at[z], zg.at[z], zg_s.at[i], zg_r.at[i], z=around(z, i, NZ))

    def c_ygather():
        for i in range(1, NZ):
            arrived(zg.at[around(z, -i, NZ)], zg_r.at[i])
        lines = jnp.zeros((4, 128), F32)
        for k in range(NZ):
            chunk = zg[k].astype(F32)
            q, r = divmod(k, 4)
            nat[8 * q:8 * q + 8, VC + 128 * r:VC + 128 * r + 128] = chunk[0:8]
            q, r = divmod(k, 2)
            nat[4 * q:4 * q + 4, 128 * r:128 * r + 128] = chunk[8:12]
            lines = lines + chunk[12:16]
        yg[y] = nat[...].astype(BF)
        for i in range(1, NY):
            send(yg.at[y], yg.at[y], yg_s.at[i], yg_r.at[i], y=around(y, i, NY))
        row = lax.broadcasted_iota(jnp.int32, (8, 128), 0)
        st[...] = jnp.where(row < 4, lines[0:1] + lines[1:2], lines[2:3] + lines[3:4])
        for i in range(1, NT):
            send(st, sr.at[i], sc_s.at[i], sc_r.at[i], tp=around(t, i, NT))

    def c_squares():
        for i in range(1, NT):
            arrived(sr.at[i], sc_r.at[i])
        total = st[...]
        for i in range(1, NT):
            total = total + sr[i]
        sy[...] = total
        for i in range(1, NY):
            send(sy, syr.at[i], sy_s.at[i], sy_r.at[i], y=around(y, i, NY))

    def c_moments():
        for i in range(1, NY):
            arrived(yg.at[around(y, -i, NY)], yg_r.at[i])
        whole = yg[...].reshape(R, PC).astype(F32)
        vmb[...], vsb[...], vn_out[...] = moments(vmb[...], vsb[...], whole[:, 0:VC])
        omb[...], osb[...], on_out[...] = moments(omb[...], osb[...], whole[:, VC:PC])

    def c_scales():
        for i in range(1, NY):
            arrived(syr.at[i], sy_r.at[i])
        total = sy[...]
        for i in range(1, NY):
            total = total + syr[i]
        row = lax.broadcasted_iota(jnp.int32, (8, 128), 0)
        mean = jnp.sum(total, axis=1, keepdims=True) * jnp.where(row < 4, 1.0 / (R * WIDTH), 1.0 / (R * D))
        scales[...] = lax.rsqrt(mean + FLOOR)

    for c in loads[0:2]:
        c.wait()
    g[z, y, 0:VROWS, :] = vwb[...].astype(BF)
    g[z, y, VROWS:VROWS + OROWS, :] = owb[:, 0:VC].astype(BF)
    g[z, y, VROWS + OROWS:BLK, :] = owb[:, VC:OC].astype(BF)
    pl.semaphore_wait(barrier, NT + NY)
    a_begin()
    b_ring(0)
    c_partial(1)
    c_scatter(1)
    c_partial(0)
    c_scatter(0)
    b_ring(1)
    a_ring(0, 0)
    a_ring(0, 1)
    token()
    token()
    b_ring(2)
    token()
    c_gather(1)
    c_gather(0)
    b_forward(0)
    a_ring(1, 0)
    a_ring(1, 1)
    b_ring(3)
    token()
    token()
    c_project(1)
    c_project(0)
    token()
    token()
    a_ring(2, 0)
    a_ring(2, 1)
    b_ring(4)
    b_forward(1)
    c_zscatter()
    a_ring(3, 0)
    a_ring(3, 1)
    b_ring(5)
    b_forward(2)
    a_ring(4, 0)
    a_ring(4, 1)
    b_ring(6)
    b_forward(3)
    c_zgather()
    a_ring(5, 0)
    a_ring(5, 1)
    b_ring(7)
    b_forward(4)
    a_ring(6, 0)
    a_ring(6, 1)
    b_ring(8)
    b_forward(5)
    c_ygather()
    a_ring(7, 0)
    a_ring(7, 1)
    b_forward(6)
    b_forward(7)
    c_squares()
    b_forward(8)
    c_moments()
    c_scales()
    a_ring(8, 0)
    a_ring(8, 1)
    for s in range(LAST + 1):
        b_end(s)
    for c in loads[12:]:
        c.wait()
    for c in sent:
        c.wait_send()


def update_kernel(
    g, scales, vn, on, vm, vs, om, os, fv, fo, vw, ow,
    vstep_out, vnew_out, vcopy_out, vm_out, vs_out, ostep_out, onew_out, ocopy_out, om_out, os_out,
    vstep, vnew, vcopy, ostep, onew, ocopy, wsem, vcsem, ocsem,
):
    z, y = lax.axis_index("z"), lax.axis_index("y")
    row = z * NY + y
    writes = []

    def write(src, dst, sem):
        c = pltpu.make_async_copy(src, dst, sem)
        c.start()
        writes.append(c)

    for k, (src, dst) in enumerate(((vm, vm_out), (vs, vs_out), (om, om_out), (os, os_out))):
        write(src, dst, wsem.at[k])
    v_scale = scales[0:1, 0:1]
    o_scale = scales[4:5, 0:1]

    def two(normalized, scale):
        scaled = normalized * (scale * STEP_RATE)
        high = scaled.astype(BF)
        low = (scaled - high.astype(F32)).astype(BF)
        return jnp.concatenate([high, low], axis=0)

    v_two = two(vn[...], v_scale)
    o_two = two(on[...], o_scale)
    vt, ot = NY * VROWS, NY * OROWS
    for k in range(NZ):
        f = fv[k * vt:(k + 1) * vt, :]
        delta = jnp.dot(jnp.concatenate([f, f], axis=1), v_two, preferred_element_type=F32)
        held = g[k, :, 0:VROWS, :].reshape(vt, VC).astype(F32)
        vcopy[k * vt:(k + 1) * vt, :] = (held - delta).astype(BF)
        write(vcopy.at[pl.ds(k * vt, vt)], vcopy_out.at[pl.ds(k * vt, vt)], vcsem.at[k])
        f = fo[k * ot:(k + 1) * ot, :]
        delta = jnp.dot(jnp.concatenate([f, f], axis=1), o_two, preferred_element_type=F32)
        for h in range(2):
            lo = VROWS + h * OROWS
            held = g[k, :, lo:lo + OROWS, :].reshape(ot, VC).astype(F32)
            ocopy[k * ot:(k + 1) * ot, h * VC:(h + 1) * VC] = (held - delta[:, h * VC:(h + 1) * VC]).astype(BF)
        write(ocopy.at[pl.ds(k * ot, ot)], ocopy_out.at[pl.ds(k * ot, ot)], ocsem.at[k])
    highest = lax.Precision.HIGHEST
    v_here = fv[pl.ds(pl.multiple_of(row * VROWS, VROWS), VROWS), :].astype(F32)
    o_here = fo[pl.ds(pl.multiple_of(row * OROWS, OROWS), OROWS), :].astype(F32)
    vstep[...] = v_scale * jnp.dot(v_here, vn[...], precision=highest, preferred_element_type=F32)
    ostep[...] = o_scale * jnp.dot(o_here, on[...], precision=highest, preferred_element_type=F32)
    vnew[...] = vw[...] - STEP_RATE * vstep[...]
    onew[...] = ow[...] - STEP_RATE * ostep[...]
    for k, (src, dst) in enumerate(((vstep, vstep_out), (vnew, vnew_out), (ostep, ostep_out), (onew, onew_out))):
        write(src, dst, wsem.at[4 + k])
    for c in writes:
        c.wait()


def per_device(
    normed_input, value_cotangent, mixer_output, output_cotangent, value_factor, output_factor,
    value_master, value_moment, value_second, output_master, output_moment, output_second,
):
    anywhere = pl.BlockSpec(memory_space=pl.ANY)
    inside = pl.BlockSpec(memory_space=pltpu.VMEM)
    dma = pltpu.SemaphoreType.DMA

    def vmem(shape, dtype):
        return pltpu.VMEM(shape, dtype)

    handed = (
        vmem((NZ, NY, BLK, VC), BF), vmem((8, 128), F32), vmem((R, VC), F32), vmem((R, OC), F32),
        vmem((R, VC), F32), vmem((R, VC), F32), vmem((R, OC), F32), vmem((R, OC), F32),
        vmem((D, R), BF), vmem((WIDTH, R), BF), vmem((VROWS, VC), F32), vmem((OROWS, OC), F32),
    )
    state = pl.pallas_call(
        exchange_kernel,
        name="exchange",
        out_shape=handed,
        in_specs=[anywhere] * 12,
        out_specs=(inside,) * len(handed),
        scratch_shapes=[
            vmem((TOK, FEAT), BF), vmem((TOK, VC), BF), vmem((TOK, HEAD), BF), vmem((TOK, OC), BF),
            vmem((FEAT, R), BF), vmem((HEAD, R), BF),
            vmem((2, NT, 16, TOK), BF), vmem((2, NT, 16, TOK), BF), vmem((2, NT, 16, TOK), BF),
            vmem((NY, R // NY, VC), F32), vmem((NY, R // NY, OC), F32),
            vmem((NY, R // NY, VC), BF), vmem((NY, R // NY, OC), BF),
            vmem((NY, R // NY, VC), BF), vmem((NY, R // NY, OC), BF),
            vmem((NZ, 16, 128), F32), vmem((NZ, 16, 128), BF), vmem((NZ, 16, 128), BF), vmem((NZ, 16, 128), BF),
            vmem((R // NY, PC), F32), vmem((NY, R // NY, PC), BF),
            vmem((8, 128), F32), vmem((NT, 8, 128), F32), vmem((8, 128), F32), vmem((NY, 8, 128), F32),
            dma((14,)), pltpu.SemaphoreType.REGULAR((2,)),
            dma((2, NT)), dma((2, NT)), dma((2, NT)), dma((2, NT)), dma((NT,)), dma((NT,)), dma((NY,)), dma((NY,)),
            dma((2, NY)), dma((2, NY)), dma((NY,)), dma((NY,)),
            dma((NZ,)), dma((NZ,)), dma((NZ,)), dma((NZ,)),
            dma((NY,)), dma((NY,)),
            dma((2, 2, NZ // 2 + 1)), dma((2, 2, NZ // 2 + 1)), dma((2, NZ // 2 + 1)), dma((2, NZ // 2 + 1)),
            dma((4, NZ)), dma((4, NZ)),
        ],
        compiler_params=pltpu.CompilerParams(collective_id=0, has_side_effects=True, vmem_limit_bytes=59_900_000),
    )(
        normed_input, value_cotangent, mixer_output, output_cotangent, value_factor, output_factor,
        value_master, value_moment, value_second, output_master, output_moment, output_second,
    )

    def like(a, dtype=F32):
        return jax.ShapeDtypeStruct(a, dtype)

    return pl.pallas_call(
        update_kernel,
        name="update",
        out_shape=(
            like((VROWS, VC)), like((VROWS, VC)), like((D, VC), BF), like((R, VC)), like((R, VC)),
            like((OROWS, OC)), like((OROWS, OC)), like((WIDTH, OC), BF), like((R, OC)), like((R, OC)),
        ),
        in_specs=[inside] * len(handed),
        out_specs=(anywhere,) * 10,
        scratch_shapes=[
            vmem((VROWS, VC), F32), vmem((VROWS, VC), F32), vmem((D, VC), BF),
            vmem((OROWS, OC), F32), vmem((OROWS, OC), F32), vmem((WIDTH, OC), BF),
            dma((8,)), dma((NZ,)), dma((NZ,)),
        ],
        compiler_params=pltpu.CompilerParams(vmem_limit_bytes=30 << 20),
    )(*state)


def solution(mesh):
    finer = Mesh(mesh.devices.reshape(NZ, NY, NT), ("z", "y", "tp"))
    fs = ("z", "y")
    rows, cols = P(fs, "tp"), P(None, "tp")
    return jax.shard_map(
        per_device,
        mesh=finer,
        in_specs=(rows, rows, rows, rows, P(), P(), rows, cols, cols, rows, cols, cols),
        out_specs=(rows, rows, cols, cols, cols, rows, rows, cols, cols, cols),
        check_vma=False,
    )
```

```python
import jax
import jax.numpy as jnp
from jax import lax
from jax.experimental import pallas as pl
from jax.experimental.pallas import tpu as pltpu
from jax.sharding import Mesh
from jax.sharding import PartitionSpec as P

D = 4096
WIDTH = 2048
R = 128
TOK = 512
NZ, NY, NT = 16, 4, 8
FEAT = D // NT
HEAD = WIDTH // NT
VC = WIDTH // NT
OC = D // NT
PC = VC + OC
VROWS = D // (NZ * NY)
OROWS = WIDTH // (NZ * NY)
BLK = VROWS + 2 * OROWS
ASPLIT = 16
BHALF = 64
REACH = 2

BETA_ONE = 0.8
BETA_TWO = 0.9
EPSILON = 1e-08
STEP_RATE = 0.005
FLOOR = 0.25

BF = jnp.bfloat16
F32 = jnp.float32
MESH = pl.DeviceIdType.MESH


def moments(first, second, projected):
    first_new = BETA_ONE * first + (1.0 - BETA_ONE) * projected
    second_new = BETA_TWO * second + (1.0 - BETA_TWO) * projected * projected
    normalized = first_new / (jnp.sqrt(second_new) + EPSILON)
    return first_new, second_new, normalized


def exchange_kernel(
    n_in, vc_in, mo_in, oc_in, fv_in, fo_in, vw_in, vm_in, vs_in, ow_in, om_in, os_in,
    g, scales, vn_out, on_out, vmb, vsb, omb, osb, fv_all, fo_all, vwb, owb,
    nb, vcb, mob, ocb, fvb, fob,
    xs, xr, xg, pfv, pfo, pbv, pbo, yrv, yro, zs, zb, zr, zg, nat, yg, st, sr, sy, syr,
    lsem, tok,
    xs_s, xs_r, xg_s, xg_r, sc_s, sc_r, sy_s, sy_r, yr_s, yr_r, yg_s, yg_r,
    zr_s, zr_r, zg_s, zg_r, ay_s, ay_r, az_s, az_r, bz_s, bz_r, by_s, by_r,
):
    z, y, t = lax.axis_index("z"), lax.axis_index("y"), lax.axis_index("tp")

    def around(k, i, n):
        return lax.rem(k + (i + n), n)

    up, down = around(z, 1, NZ), around(z, -1, NZ)
    yup, ydown = around(y, 1, NY), around(y, -1, NY)

    barrier = pltpu.get_barrier_semaphore()
    for i in range(1, NT):
        pl.semaphore_signal(barrier, inc=1, device_id={"tp": around(t, i, NT)}, device_id_type=MESH)
    for i in range(1, NY):
        pl.semaphore_signal(barrier, inc=1, device_id={"y": around(y, i, NY)}, device_id_type=MESH)
    for i in range(1, REACH + 1):
        for k in (i, -i):
            pl.semaphore_signal(barrier, inc=1, device_id={"z": around(z, k, NZ)}, device_id_type=MESH)

    loads = []
    for k, (src, dst) in enumerate((
        (vw_in, vwb), (ow_in, owb),
        (fo_in.at[pl.ds(pl.multiple_of(t * HEAD, HEAD), HEAD)], fob), (mo_in, mob),
        (fv_in.at[pl.ds(pl.multiple_of(t * FEAT, FEAT), FEAT)], fvb), (n_in, nb),
        (oc_in, ocb), (vc_in, vcb),
        (vm_in, vmb), (vs_in, vsb), (om_in, omb), (os_in, osb),
        (fv_in, fv_all), (fo_in, fo_all),
    )):
        c = pltpu.make_async_copy(src, dst, lsem.at[k])
        c.start()
        loads.append(c)

    sent = []

    def remote(src, dst, ssem, rsem, **where):
        return pltpu.make_async_remote_copy(
            src_ref=src, dst_ref=dst, send_sem=ssem, recv_sem=rsem,
            device_id=where, device_id_type=MESH,
        )

    def send(src, dst, ssem, rsem, **where):
        c = remote(src, dst, ssem, rsem, **where)
        c.start()
        sent.append(c)

    def arrived(dst, rsem):
        remote(dst, dst, rsem, rsem, tp=t).wait_recv()

    def a_rows(k, h):
        return g.at[k, pl.ds(h * (NY // 2), NY // 2), pl.ds(0, ASPLIT), :]

    def b_rows(k, j=None, part=None):
        lo, hi = {None: (ASPLIT, BLK), 0: (ASPLIT, BHALF), 1: (BHALF, BLK)}[part]
        return g.at[k, y if j is None else j, pl.ds(lo, hi - lo), :]

    LAST = NZ // 2

    def a_begin():
        own = g.at[z, y, pl.ds(0, ASPLIT), :]
        for i in range(1, NY):
            send(own, own, ay_s.at[i], ay_r.at[i], y=around(y, i, NY))

    def a_ring(s, h):
        if s == 0 and h == 0:
            for i in range(1, NY):
                arrived(g.at[z, around(y, -i, NY), pl.ds(0, ASPLIT), :], ay_r.at[i])
        for d, (k, to) in enumerate(((around(z, -s, NZ), up), (around(z, s, NZ), down))):
            if 0 < s < LAST or (s == LAST and d == h):
                arrived(a_rows(k, h), az_r.at[d, h, s])
            if s + 1 < LAST or (s + 1 == LAST and d == h):
                send(a_rows(k, h), a_rows(k, h), az_s.at[d, h, s + 1], az_r.at[d, h, s + 1], z=to)

    def b_across(k, b):
        block = b_rows(k)
        send(block, block, by_s.at[0, b], by_r.at[0, b], y=yup)
        send(block, block, by_s.at[1, b], by_r.at[1, b], y=ydown)

    def b_ids(s):
        if s == 0:
            return ((0, 0),)
        if s == LAST:
            return ((LAST, NZ - 1),)
        return ((-s, 2 * s - 1), (s, 2 * s))

    def b_ring(s):
        for h in range(2):
            for d, (k, to) in enumerate(((around(z, -s, NZ), up), (around(z, s, NZ), down))):
                block = b_rows(k, part=h)
                if 0 < s < LAST or (s == LAST and d == h):
                    arrived(block, bz_r.at[d, h, s])
                if s + 1 < LAST or (s + 1 == LAST and d == h):
                    send(block, block, bz_s.at[d, h, s + 1], bz_r.at[d, h, s + 1], z=to)
        for off, b in b_ids(s):
            b_across(around(z, off, NZ), b)

    def b_forward(s):
        for off, b in b_ids(s):
            k = around(z, off, NZ)
            arrived(b_rows(k, ydown), by_r.at[0, b])
            block = b_rows(k, ydown, 0)
            send(block, block, by_s.at[2, b], by_r.at[2, b], y=yup)
            arrived(b_rows(k, yup), by_r.at[1, b])
            block = b_rows(k, yup, 1)
            send(block, block, by_s.at[3, b], by_r.at[3, b], y=ydown)

    def b_end(s):
        across = around(y, 2, NY)
        for off, b in b_ids(s):
            k = around(z, off, NZ)
            arrived(b_rows(k, across, 0), by_r.at[2, b])
            arrived(b_rows(k, across, 1), by_r.at[3, b])

    def token(k):
        if k > 0:
            pl.semaphore_wait(tok.at[0], 1)
            pl.semaphore_wait(tok.at[1], 1)
        if REACH * (k + 1) < LAST:
            for j, i in enumerate((REACH, -REACH)):
                pl.semaphore_signal(tok.at[j], inc=1, device_id={"z": around(z, i, NZ)}, device_id_type=MESH)

    nt = (((1,), (1,)), ((), ()))

    def c_partial(w):
        for c in loads[4 - 2 * w:6 - 2 * w]:
            c.wait()
        factor, rows = (fob, mob) if w else (fvb, nb)
        part = lax.dot_general(factor[...].T, rows[...], nt, preferred_element_type=F32)
        xs[w] = part.astype(BF).reshape(NT, 16, TOK)

    def c_scatter(w):
        for i in range(1, NT):
            to = around(t, i, NT)
            send(xs.at[w, to], xr.at[w, i], xs_s.at[w, i], xs_r.at[w, i], tp=to)

    def c_gather(w):
        for i in range(1, NT):
            arrived(xr.at[w, i], xs_r.at[w, i])
        total = xs[w, t].astype(F32)
        for i in range(1, NT):
            total = total + xr[w, i].astype(F32)
        xg[w, t] = total.astype(BF)
        for i in range(1, NT):
            send(xg.at[w, t], xg.at[w, t], xg_s.at[w, i], xg_r.at[w, i], tp=around(t, i, NT))

    def c_project(w):
        loads[7 - w].wait()
        for i in range(1, NT):
            arrived(xg.at[w, around(t, -i, NT)], xg_r.at[w, i])
        right, whole, rounded, landing = (ocb, pfo, pbo, yro) if w else (vcb, pfv, pbv, yrv)
        p = jnp.dot(xg[w].reshape(R, TOK), right[...], preferred_element_type=F32)
        p = p.reshape(NY, R // NY, p.shape[-1])
        whole[...] = p
        rounded[...] = p.astype(BF)
        for i in range(1, NY):
            to = around(y, i, NY)
            send(rounded.at[to], landing.at[i], yr_s.at[w, i], yr_r.at[w, i], y=to)

    def c_zscatter():
        for i in range(1, NY):
            arrived(yro.at[i], yr_r.at[1, i])
        total = pfo[y]
        for i in range(1, NY):
            total = total + yro[i].astype(F32)
        for k in range(NZ):
            q, r = divmod(k, 4)
            zs[k, 0:8, :] = total[8 * q:8 * q + 8, 128 * r:128 * r + 128]
        for i in range(1, NY):
            arrived(yrv.at[i], yr_r.at[0, i])
        total = pfv[y]
        for i in range(1, NY):
            total = total + yrv[i].astype(F32)
        for k in range(NZ):
            q, r = divmod(k, 2)
            zs[k, 8:12, :] = total[4 * q:4 * q + 4, 128 * r:128 * r + 128]
            zs[k, 12:16, :] = jnp.zeros((4, 128), F32)
        zb[...] = zs[...].astype(BF)
        for i in range(1, NZ):
            to = around(z, i, NZ)
            send(zb.at[to], zr.at[i], zr_s.at[i], zr_r.at[i], z=to)

    def c_zgather():
        for c in loads[8:12]:
            c.wait()
        down8 = pl.multiple_of(y * (R // NY) + 8 * (z // 4), 8)
        o_cols = pl.ds(pl.multiple_of(128 * lax.rem(z, 4), 128), 128)
        v_cols = pl.ds(pl.multiple_of(128 * lax.rem(z, 2), 128), 128)
        rows8 = pl.ds(down8, 8)
        om, osq = omb[rows8, o_cols], osb[rows8, o_cols]
        vm, vsq = vmb[rows8, v_cols], vsb[rows8, v_cols]
        second = lax.rem(z // 2, 2) == 1
        vm = jnp.where(second, vm[4:8], vm[0:4])
        vsq = jnp.where(second, vsq[4:8], vsq[0:4])
        for i in range(1, NZ):
            arrived(zr.at[i], zr_r.at[i])
        total = zs[z]
        for i in range(1, NZ):
            total = total + zr[i].astype(F32)
        held = total.astype(BF).astype(F32)
        _, _, on = moments(om, osq, held[0:8])
        _, _, vn = moments(vm, vsq, held[8:12])
        o_sum = jnp.sum(on * on, axis=0, keepdims=True)
        v_sum = jnp.sum(vn * vn, axis=0, keepdims=True)
        o_high, v_high = o_sum.astype(BF).astype(F32), v_sum.astype(BF).astype(F32)
        row = lax.broadcasted_iota(jnp.int32, (16, 128), 0)
        for k, line in enumerate((v_high, v_sum - v_high, o_high, o_sum - o_high)):
            total = jnp.where(row == 12 + k, line, total)
        zg[z] = total.astype(BF)
        for i in range(1, NZ):
            send(zg.at[z], zg.at[z], zg_s.at[i], zg_r.at[i], z=around(z, i, NZ))

    def c_ygather():
        for i in range(1, NZ):
            arrived(zg.at[around(z, -i, NZ)], zg_r.at[i])
        lines = jnp.zeros((4, 128), F32)
        for k in range(NZ):
            chunk = zg[k].astype(F32)
            q, r = divmod(k, 4)
            nat[8 * q:8 * q + 8, VC + 128 * r:VC + 128 * r + 128] = chunk[0:8]
            q, r = divmod(k, 2)
            nat[4 * q:4 * q + 4, 128 * r:128 * r + 128] = chunk[8:12]
            lines = lines + chunk[12:16]
        yg[y] = nat[...].astype(BF)
        for i in range(1, NY):
            send(yg.at[y], yg.at[y], yg_s.at[i], yg_r.at[i], y=around(y, i, NY))
        row = lax.broadcasted_iota(jnp.int32, (8, 128), 0)
        st[...] = jnp.where(row < 4, lines[0:1] + lines[1:2], lines[2:3] + lines[3:4])
        for i in range(1, NT):
            send(st, sr.at[i], sc_s.at[i], sc_r.at[i], tp=around(t, i, NT))

    def c_squares():
        for i in range(1, NT):
            arrived(sr.at[i], sc_r.at[i])
        total = st[...]
        for i in range(1, NT):
            total = total + sr[i]
        sy[...] = total
        for i in range(1, NY):
            send(sy, syr.at[i], sy_s.at[i], sy_r.at[i], y=around(y, i, NY))

    def c_moments():
        for i in range(1, NY):
            arrived(yg.at[around(y, -i, NY)], yg_r.at[i])
        whole = yg[...].reshape(R, PC).astype(F32)
        vmb[...], vsb[...], vn_out[...] = moments(vmb[...], vsb[...], whole[:, 0:VC])
        omb[...], osb[...], on_out[...] = moments(omb[...], osb[...], whole[:, VC:PC])

    def c_scales():
        for i in range(1, NY):
            arrived(syr.at[i], sy_r.at[i])
        total = sy[...]
        for i in range(1, NY):
            total = total + syr[i]
        row = lax.broadcasted_iota(jnp.int32, (8, 128), 0)
        mean = jnp.sum(total, axis=1, keepdims=True) * jnp.where(row < 4, 1.0 / (R * WIDTH), 1.0 / (R * D))
        scales[...] = lax.rsqrt(mean + FLOOR)

    for c in loads[0:2]:
        c.wait()
    g[z, y, 0:VROWS, :] = vwb[...].astype(BF)
    g[z, y, VROWS:VROWS + OROWS, :] = owb[:, 0:VC].astype(BF)
    g[z, y, VROWS + OROWS:BLK, :] = owb[:, VC:OC].astype(BF)
    pl.semaphore_wait(barrier, NT + NY - 2 + 2 * REACH)
    token(0)
    a_begin()
    b_ring(0)
    c_partial(1)
    c_scatter(1)
    c_partial(0)
    c_scatter(0)
    token(1)
    b_ring(1)
    a_ring(0, 0)
    a_ring(0, 1)
    token(2)
    b_ring(2)
    c_gather(1)
    c_gather(0)
    b_forward(0)
    a_ring(1, 0)
    a_ring(1, 1)
    b_ring(3)
    c_project(1)
    c_project(0)
    a_ring(2, 0)
    a_ring(2, 1)
    b_ring(4)
    b_forward(1)
    token(3)
    c_zscatter()
    a_ring(3, 0)
    a_ring(3, 1)
    b_ring(5)
    b_forward(2)
    a_ring(4, 0)
    a_ring(4, 1)
    b_ring(6)
    b_forward(3)
    c_zgather()
    a_ring(5, 0)
    a_ring(5, 1)
    b_ring(7)
    b_forward(4)
    a_ring(6, 0)
    a_ring(6, 1)
    b_forward(5)
    c_ygather()
    b_ring(8)
    a_ring(7, 0)
    a_ring(7, 1)
    b_forward(6)
    b_forward(7)
    c_squares()
    b_forward(8)
    c_moments()
    c_scales()
    a_ring(8, 0)
    a_ring(8, 1)
    for s in range(LAST + 1):
        b_end(s)
    for c in loads[12:]:
        c.wait()
    for c in sent:
        c.wait_send()


def update_kernel(
    g, scales, vn, on, vm, vs, om, os, fv, fo, vw, ow,
    vstep_out, vnew_out, vcopy_out, vm_out, vs_out, ostep_out, onew_out, ocopy_out, om_out, os_out,
    vstep, vnew, vcopy, ostep, onew, ocopy, wsem, vcsem, ocsem,
):
    z, y = lax.axis_index("z"), lax.axis_index("y")
    row = z * NY + y
    writes = []

    def write(src, dst, sem):
        c = pltpu.make_async_copy(src, dst, sem)
        c.start()
        writes.append(c)

    for k, (src, dst) in enumerate(((vm, vm_out), (vs, vs_out), (om, om_out), (os, os_out))):
        write(src, dst, wsem.at[k])
    v_scale = scales[0:1, 0:1]
    o_scale = scales[4:5, 0:1]

    def two(normalized, scale):
        scaled = normalized * (scale * STEP_RATE)
        high = scaled.astype(BF)
        low = (scaled - high.astype(F32)).astype(BF)
        return jnp.concatenate([high, low], axis=0)

    v_two = two(vn[...], v_scale)
    o_two = two(on[...], o_scale)
    vt, ot = NY * VROWS, NY * OROWS
    for k in range(NZ):
        f = fv[k * vt:(k + 1) * vt, :]
        delta = jnp.dot(jnp.concatenate([f, f], axis=1), v_two, preferred_element_type=F32)
        held = g[k, :, 0:VROWS, :].reshape(vt, VC).astype(F32)
        vcopy[k * vt:(k + 1) * vt, :] = (held - delta).astype(BF)
        write(vcopy.at[pl.ds(k * vt, vt)], vcopy_out.at[pl.ds(k * vt, vt)], vcsem.at[k])
        f = fo[k * ot:(k + 1) * ot, :]
        delta = jnp.dot(jnp.concatenate([f, f], axis=1), o_two, preferred_element_type=F32)
        for h in range(2):
            lo = VROWS + h * OROWS
            held = g[k, :, lo:lo + OROWS, :].reshape(ot, VC).astype(F32)
            ocopy[k * ot:(k + 1) * ot, h * VC:(h + 1) * VC] = (held - delta[:, h * VC:(h + 1) * VC]).astype(BF)
        write(ocopy.at[pl.ds(k * ot, ot)], ocopy_out.at[pl.ds(k * ot, ot)], ocsem.at[k])
    highest = lax.Precision.HIGHEST
    v_here = fv[pl.ds(pl.multiple_of(row * VROWS, VROWS), VROWS), :].astype(F32)
    o_here = fo[pl.ds(pl.multiple_of(row * OROWS, OROWS), OROWS), :].astype(F32)
    vstep[...] = v_scale * jnp.dot(v_here, vn[...], precision=highest, preferred_element_type=F32)
    ostep[...] = o_scale * jnp.dot(o_here, on[...], precision=highest, preferred_element_type=F32)
    vnew[...] = vw[...] - STEP_RATE * vstep[...]
    onew[...] = ow[...] - STEP_RATE * ostep[...]
    for k, (src, dst) in enumerate(((vstep, vstep_out), (vnew, vnew_out), (ostep, ostep_out), (onew, onew_out))):
        write(src, dst, wsem.at[4 + k])
    for c in writes:
        c.wait()


def per_device(
    normed_input, value_cotangent, mixer_output, output_cotangent, value_factor, output_factor,
    value_master, value_moment, value_second, output_master, output_moment, output_second,
):
    anywhere = pl.BlockSpec(memory_space=pl.ANY)
    inside = pl.BlockSpec(memory_space=pltpu.VMEM)
    dma = pltpu.SemaphoreType.DMA

    def vmem(shape, dtype):
        return pltpu.VMEM(shape, dtype)

    handed = (
        vmem((NZ, NY, BLK, VC), BF), vmem((8, 128), F32), vmem((R, VC), F32), vmem((R, OC), F32),
        vmem((R, VC), F32), vmem((R, VC), F32), vmem((R, OC), F32), vmem((R, OC), F32),
        vmem((D, R), BF), vmem((WIDTH, R), BF), vmem((VROWS, VC), F32), vmem((OROWS, OC), F32),
    )
    state = pl.pallas_call(
        exchange_kernel,
        name="exchange",
        out_shape=handed,
        in_specs=[anywhere] * 12,
        out_specs=(inside,) * len(handed),
        scratch_shapes=[
            vmem((TOK, FEAT), BF), vmem((TOK, VC), BF), vmem((TOK, HEAD), BF), vmem((TOK, OC), BF),
            vmem((FEAT, R), BF), vmem((HEAD, R), BF),
            vmem((2, NT, 16, TOK), BF), vmem((2, NT, 16, TOK), BF), vmem((2, NT, 16, TOK), BF),
            vmem((NY, R // NY, VC), F32), vmem((NY, R // NY, OC), F32),
            vmem((NY, R // NY, VC), BF), vmem((NY, R // NY, OC), BF),
            vmem((NY, R // NY, VC), BF), vmem((NY, R // NY, OC), BF),
            vmem((NZ, 16, 128), F32), vmem((NZ, 16, 128), BF), vmem((NZ, 16, 128), BF), vmem((NZ, 16, 128), BF),
            vmem((R // NY, PC), F32), vmem((NY, R // NY, PC), BF),
            vmem((8, 128), F32), vmem((NT, 8, 128), F32), vmem((8, 128), F32), vmem((NY, 8, 128), F32),
            dma((14,)), pltpu.SemaphoreType.REGULAR((2,)),
            dma((2, NT)), dma((2, NT)), dma((2, NT)), dma((2, NT)), dma((NT,)), dma((NT,)), dma((NY,)), dma((NY,)),
            dma((2, NY)), dma((2, NY)), dma((NY,)), dma((NY,)),
            dma((NZ,)), dma((NZ,)), dma((NZ,)), dma((NZ,)),
            dma((NY,)), dma((NY,)),
            dma((2, 2, NZ // 2 + 1)), dma((2, 2, NZ // 2 + 1)), dma((2, 2, NZ // 2 + 1)), dma((2, 2, NZ // 2 + 1)),
            dma((4, NZ)), dma((4, NZ)),
        ],
        compiler_params=pltpu.CompilerParams(collective_id=0, has_side_effects=True, vmem_limit_bytes=59_900_000),
    )(
        normed_input, value_cotangent, mixer_output, output_cotangent, value_factor, output_factor,
        value_master, value_moment, value_second, output_master, output_moment, output_second,
    )

    def like(a, dtype=F32):
        return jax.ShapeDtypeStruct(a, dtype)

    return pl.pallas_call(
        update_kernel,
        name="update",
        out_shape=(
            like((VROWS, VC)), like((VROWS, VC)), like((D, VC), BF), like((R, VC)), like((R, VC)),
            like((OROWS, OC)), like((OROWS, OC)), like((WIDTH, OC), BF), like((R, OC)), like((R, OC)),
        ),
        in_specs=[inside] * len(handed),
        out_specs=(anywhere,) * 10,
        scratch_shapes=[
            vmem((VROWS, VC), F32), vmem((VROWS, VC), F32), vmem((D, VC), BF),
            vmem((OROWS, OC), F32), vmem((OROWS, OC), F32), vmem((WIDTH, OC), BF),
            dma((8,)), dma((NZ,)), dma((NZ,)),
        ],
        compiler_params=pltpu.CompilerParams(vmem_limit_bytes=30 << 20),
    )(*state)


def solution(mesh):
    finer = Mesh(mesh.devices.reshape(NZ, NY, NT), ("z", "y", "tp"))
    fs = ("z", "y")
    rows, cols = P(fs, "tp"), P(None, "tp")
    return jax.shard_map(
        per_device,
        mesh=finer,
        in_specs=(rows, rows, rows, rows, P(), P(), rows, cols, cols, rows, cols, cols),
        out_specs=(rows, rows, cols, cols, cols, rows, rows, cols, cols, cols),
        check_vma=False,
    )
```
